512 devices in a mesh: grp: 2 (over y), sp: 32 (over z, core), tp: 8 (over x).
Axes of the slice: x: 8, y: 2, z: 16, core: 2. Of those that a mesh axis runs over, the one named last changes fastest.
The devices are a block of a 8x8x16 slice.
Arguments:
- residual: bfloat16 [16384, 2048], P(('grp', 'sp')), parts along dimension 0, may hold values from -34 to 34
- queries: bfloat16 [16384, 1024], P(('grp', 'sp'), 'tp'), parts along dimension 0, may hold values from -400 to 400
- keys: bfloat16 [16384, 512], P(('grp', 'sp'), 'tp'), parts along dimension 0, may hold values from -8 to 8
- values: bfloat16 [16384, 512], P(('grp', 'sp'), 'tp'), parts along dimension 0, may hold values from -6 to 6
- segments: int32 [16384], P(('grp', 'sp')), parts along dimension 0, may hold values from 0 to 16, never falling along the last dimension, each value on 1 to 768 neighbouring positions
- routes: int32 [16384, 2], P(('grp', 'sp')), parts along dimension 0, may hold values from 0 to 31, all different within a row; in each aligned block of 256 rows (0 to 255, 256 to 511, ...) at most 32 rows name the same one
- route_weight: float32 [16384, 2], P(('grp', 'sp')), parts along dimension 0, may hold values from 0.3 to 3
- sinks: float32 [16], P('tp'), may hold values from 1 to 6
- out_weight: bfloat16 [1024, 2048], P('tp'), may hold values from -1 to 1
- norm_gain: float32 [2048], replicated, may hold values from 0.1 to 1.9
- expert_gate: bfloat16 [32, 2048, 1024], P('sp', None, 'tp'), may hold values from -0.125 to 0.125
- expert_up: bfloat16 [32, 2048, 1024], P('sp', None, 'tp'), may hold values from -0.125 to 0.125
- expert_down: bfloat16 [32, 1024, 2048], P('sp', None, 'tp'), may hold values from -0.1875 to 0.1875
- shared_gate: bfloat16 [2048, 1024], P(None, 'tp'), may hold values from -0.125 to 0.125
- shared_up: bfloat16 [2048, 1024], P(None, 'tp'), may hold values from -0.125 to 0.125
- shared_down: bfloat16 [1024, 2048], P(None, 'tp'), may hold values from -0.1875 to 0.1875
Outputs:
- mixed: bfloat16 [16384, 2048], P(('grp', 'sp'), 'tp'), parts along dimension 0
The draws below stay inside these ranges and needn't reach their ends.
There are 2 independent parts, one for each index of `grp`. The reference program is written for one: setup_inputs(seed, part) draws one part's arguments, and reference() takes and returns one part's arrays. A program takes and returns all parts, laid end to end along the dimension named above; an argument that names none is the same for every part. Nothing has to cross between parts.
Inputs may be any that keep to these rules, and one draw needn't show every extreme that they name: `routes`: each row names 2 different experts. In the rows of one device no expert is named by more than 32 rows, and in some device's rows an expert is named by exactly 32. `segments`: document numbers never fall along the positions; every document spans 1 to 768 positions and one spans exactly 768.
All inputs are finite; a program needn't handle non-finite values.
Results may differ from the reference program's by a relative error of at most 0.0065.
Values may be sent and summed in bfloat16 or wider, within the bound.
A program may use at most 64 MiB of HBM per device.

```python
import math
import jax
import jax.numpy as jnp
import numpy as np
from jax import lax

D = 2048
HEADS = 16
KV_HEADS = 8
HEAD_DIM = 64
WINDOW = 128
EFF = 1024
SFF = 1024
TOPK = 2
TOK = 256
TOKENS = 8192
EXPERTS = 32
CAP = 32
DOCS = 17
LONGEST = 768
N_SP = 32


def query_key_pair(key):
    query_seed = jax.random.fold_in(key, 101)
    key_seed = jax.random.fold_in(key, 202)
    queries = jnp.clip(jax.random.normal(query_seed, (TOKENS, HEADS * HEAD_DIM), jnp.float32), -6.0, 6.0)
    key_rows = jnp.clip(jax.random.normal(key_seed, (TOKENS, KV_HEADS * HEAD_DIM), jnp.float32), -6.0, 6.0)
    return (queries, key_rows)


def draw_queries(key, part):
    queries, key_rows = query_key_pair(key)
    return queries.astype(jnp.bfloat16)


def draw_keys(key, part):
    queries, key_rows = query_key_pair(key)
    return key_rows.astype(jnp.bfloat16)


def draw_residual(key, part):
    profile = jnp.exp(math.log(4.0) * jnp.arange(D, dtype=jnp.float32) / D)
    jitter = jnp.exp(jax.random.uniform(jax.random.fold_in(key, 11), (D,), jnp.float32, math.log(0.7), math.log(1.4)))
    base = jnp.clip(jax.random.normal(jax.random.fold_in(key, 14), (TOKENS, D), jnp.float32), -6.0, 6.0)
    return (base * profile * jitter).astype(jnp.bfloat16)


def level_of(own_key, shape, pieces, low, high):
    def one(dim, parts):
        heights = jax.random.uniform(jax.random.fold_in(jax.random.fold_in(own_key, 6), dim), (parts,), jnp.float32, low / len(pieces), high / len(pieces))
        return jnp.repeat(jnp.exp(heights), shape[dim] // parts).reshape((-1,) + (1,) * (len(shape) - dim - 1))

    factor_of = one(*pieces[0])
    for cut in pieces[1:]:
        factor_of = factor_of * one(*cut)
    return factor_of


def length_profile(amount, total, limit, skew):
    portions = [(1 << 20) // math.isqrt(grade ** skew) + 1 for grade in range(2, amount + 1)]
    rest, counts = total - limit - (amount - 1), [1] * (amount - 1)
    while rest > 0:
        movable = [i for i in range(amount - 1) if counts[i] < limit]
        whole, left = sum([portions[i] for i in movable]), rest
        for i in movable:
            addition = min(limit - counts[i], max(1, left * portions[i] // whole), rest)
            counts[i] = counts[i] + addition
            rest = rest - addition
    return np.array([limit] + counts)


def ragged(stream_key, count, total, reach, slope):
    if count == 2:
        one = jax.random.randint(stream_key, (), max(1, total - reach), min(reach, total - 1) + 1)
        return jnp.stack([one, total - one])
    sizes = jnp.asarray(length_profile(count, total, reach, slope), jnp.int32)
    twos = (count - 1) // 2
    source_of, taker = sizes[1:1 + 2 * twos:2], sizes[2:2 + 2 * twos:2]
    room = jnp.minimum(source_of - 1, reach - taker)
    passed = jax.random.randint(jax.random.fold_in(stream_key, 1), (twos,), 0, 1 << 20) % (room + 1)
    sizes = sizes.at[1:1 + 2 * twos:2].set(source_of - passed).at[2:2 + 2 * twos:2].set(taker + passed)
    return sizes[jax.random.permutation(jax.random.fold_in(stream_key, 2), count)]


def deal_out(key, own, number, rows, count, top, reach, lean):
    order = jax.random.permutation(key, count)
    heavy_load, usual = shares(count, rows * top, reach, lean, True), shares(count, rows * top, reach, lean, False)
    places = jnp.arange(count)

    def named(tallies, turn):
        used = int((tallies > 0).sum())
        fixed = max(1, used // 4)
        shifted = fixed + (places - fixed + turn * (used - fixed)) % max(1, count - fixed)
        return jnp.zeros((count,), jnp.int32).at[order[jnp.where(places < fixed, places, shifted)]].set(jnp.asarray(tallies, jnp.int32))

    tallies = jnp.where(number % 4 == 0, named(heavy_load, number // 4), named(usual, number - number // 4 - 1))
    mixed = jax.random.permutation(jax.random.fold_in(own, 3), count)
    source_of, taker = mixed[0:count // 2 * 2:2], mixed[1:count // 2 * 2:2]
    margin = jnp.minimum(tallies[source_of] - 1, reach - tallies[taker]) // 2
    margin = jnp.where((source_of == order[0]) | (taker == order[0]) | (tallies[taker] == 0), 0, jnp.maximum(margin, 0))
    shifted = jax.random.randint(jax.random.fold_in(own, 4), (count // 2,), 0, 1 << 20) % (margin + 1)
    tallies = tallies.at[source_of].add(-shifted).at[taker].add(shifted)
    members = jnp.searchsorted(jnp.cumsum(tallies), jnp.arange(rows * top), side="right").astype(jnp.int32)
    listing = members.reshape(top, rows).T
    listing = listing[jax.random.permutation(jax.random.fold_in(own, 1), rows)]
    turn = jax.random.randint(jax.random.fold_in(own, 2), (rows, 1), 0, top)
    return jnp.take_along_axis(listing, (jnp.arange(top)[None, :] + turn) % top, axis=1)


def shares(number_of, total, limit, skew, full):
    loads = [(1 << 20) // math.isqrt(grade ** skew) + 1 for grade in range(1, number_of + 1)]
    largest = limit if full else min(limit, max(-(-total // number_of), total * loads[0] // sum(loads)))
    least = 1 if total - largest >= number_of - 1 else 0
    counts, surplus = [largest] + [least] * (number_of - 1), total - largest - least * (number_of - 1)
    while surplus > 0:
        free = [i for i in range(1, number_of) if counts[i] < largest] or [i for i in range(1, number_of) if counts[i] < limit]
        mass, remaining = sum([loads[i] for i in free]), surplus
        for i in free:
            more = min(limit - counts[i], max(1, remaining * loads[i] // mass), surplus)
            counts[i] = counts[i] + more
            surplus = surplus - more
    return np.array(counts)


def centred(rng, extent, deviation, most, pieces=(), kind=jnp.bfloat16):
    array = jax.random.normal(rng, extent, jnp.float32) * deviation
    if len(pieces) > 0:
        array = level_of(rng, extent, pieces, -0.22, 0.18) * array
    return jnp.clip(array, min=-most, max=most).astype(kind)


def setup_inputs(seed: int = 0, part: int = 0) -> dict:
    key_of = jax.random.split(jax.random.key(seed), 17)
    part_keys = jax.random.split(jax.random.fold_in(key_of[16], part), 17)
    residual = draw_residual(jax.random.fold_in(jax.random.fold_in(key_of[16], part), 71), part)
    queries = draw_queries(jax.random.fold_in(jax.random.fold_in(key_of[16], part), 71), part)
    keys = draw_keys(jax.random.fold_in(jax.random.fold_in(key_of[16], part), 71), part)
    values = centred(part_keys[3], (TOKENS, KV_HEADS * HEAD_DIM), 1.0, 6.0, ((0, 32), (1, 8)))
    segments = jnp.searchsorted(jnp.cumsum(ragged(part_keys[4], DOCS, TOKENS, LONGEST, 2)), jnp.arange(TOKENS), side="right").astype(jnp.int32)
    routes_keys = jax.random.split(jax.random.fold_in(part_keys[5], 1), TOKENS // TOK)
    routes_turns = jax.random.permutation(jax.random.fold_in(part_keys[5], 3), TOKENS // TOK)
    routes = jax.vmap(lambda own, number: deal_out(jax.random.fold_in(part_keys[5], 2), own, number, TOK, EXPERTS, TOPK, CAP, 1))(routes_keys, routes_turns).reshape((TOKENS, TOPK))
    route_weight = jnp.clip(jnp.exp(math.log(3.0) - 2.3025851 * jax.random.uniform(part_keys[6], (TOKENS, TOPK), jnp.float32) ** level_of(part_keys[6], (TOKENS, TOPK), ((0, 32),), -0.2, 0.2)), 0.3, 3.0)
    sinks = jnp.clip(1.0 + 5.0 * jax.random.uniform(key_of[7], (HEADS,), jnp.float32) ** level_of(key_of[7], (HEADS,), ((0, 8),), -0.2, 0.2), 1.0, 6.0)
    out_weight = centred(key_of[8], (HEADS * HEAD_DIM, D), (HEADS * HEAD_DIM // 32) ** -0.5, 1.0, ((0, 8),))
    norm_gain = jnp.clip(1.0 + 0.18 * jax.random.normal(key_of[9], (D,), jnp.float32), 0.1, 1.9)
    expert_gate = centred(key_of[10], (EXPERTS, D, EFF), D ** -0.5, 0.125, ((0, 32), (2, 8)))
    expert_up = centred(key_of[11], (EXPERTS, D, EFF), D ** -0.5, 0.125, ((0, 32), (2, 8)))
    expert_down = centred(key_of[12], (EXPERTS, EFF, D), EFF ** -0.5, 0.1875, ((0, 32), (2, 8)))
    shared_gate = centred(key_of[13], (D, SFF), D ** -0.5, 0.125, ((1, 8),))
    shared_up = centred(key_of[14], (D, SFF), D ** -0.5, 0.125, ((1, 8),))
    shared_down = centred(key_of[15], (SFF, D), SFF ** -0.5, 0.1875, ((1, 8),))
    return {"residual": residual, "queries": queries, "keys": keys, "values": values, "segments": segments, "routes": routes, "route_weight": route_weight, "sinks": sinks, "out_weight": out_weight, "norm_gain": norm_gain, "expert_gate": expert_gate, "expert_up": expert_up, "expert_down": expert_down, "shared_gate": shared_gate, "shared_up": shared_up, "shared_down": shared_down}


epsilon = 1e-06

def banded(rows, fill):
    blocks = rows.shape[0] // WINDOW
    shaped = rows.reshape((blocks, WINDOW) + rows.shape[1:])
    before = jnp.concatenate([jnp.full_like(shaped[:1], fill), shaped[:-1]], axis=0)
    return jnp.concatenate([before, shaped], axis=1)

def attend(queries, keys, values, segments, sinks):
    blocks = TOKENS // WINDOW
    group_size = HEADS // KV_HEADS
    query_blocks = queries.astype(jnp.float32).reshape(blocks, WINDOW, KV_HEADS, group_size, HEAD_DIM)
    key_band = banded(keys, 0).astype(jnp.float32).reshape(blocks, 2 * WINDOW, KV_HEADS, HEAD_DIM)
    value_band = banded(values, 0).astype(jnp.float32).reshape(blocks, 2 * WINDOW, KV_HEADS, HEAD_DIM)
    segment_band = banded(segments, -1)
    query_segments = segments.reshape(blocks, WINDOW)
    scores = jnp.einsum('nqhgd,nkhd->nhgqk', query_blocks, key_band) * HEAD_DIM ** (-0.5)
    offsets = jnp.arange(WINDOW)[:, None] + WINDOW - jnp.arange(2 * WINDOW)[None, :]
    allowed = (offsets >= 0) & (offsets < WINDOW) & (query_segments[:, :, None] == segment_band[:, None, :])
    sink_logits = sinks.astype(jnp.float32).reshape(KV_HEADS, group_size)[None, :, :, None]
    masked = jnp.where(allowed[:, None, None], scores, -jnp.inf)
    top_score = jnp.maximum(lax.optimization_barrier(jnp.max(masked, axis=-1)), sink_logits)
    exp_terms = jnp.where(allowed[:, None, None], jnp.exp(scores - top_score[..., None]), 0.0)
    denominator = lax.optimization_barrier(jnp.sum(exp_terms, axis=-1)) + jnp.exp(sink_logits - top_score)
    probabilities = (exp_terms / denominator[..., None]).astype(jnp.bfloat16)
    attended = jnp.einsum('nhgqk,nkhd->nqhgd', probabilities.astype(jnp.float32), value_band)
    return attended.astype(jnp.bfloat16).reshape(TOKENS, HEADS * HEAD_DIM)

def block_slots(block_routes):
    flat_ids = block_routes.reshape(-1)
    one_hot = (flat_ids[:, None] == jnp.arange(EXPERTS, dtype=jnp.int32)[None, :]).astype(jnp.int32)
    rank_in = jnp.cumsum(one_hot, axis=0) - one_hot
    return flat_ids * CAP + lax.optimization_barrier(jnp.sum(rank_in * one_hot, axis=1))

def reference(residual, queries, keys, values, segments, routes, route_weight, sinks, out_weight, norm_gain, expert_gate, expert_up, expert_down, shared_gate, shared_up, shared_down):
    attended = attend(queries, keys, values, segments, sinks)
    projected = jnp.dot(attended, out_weight, preferred_element_type=jnp.float32)
    updated = (residual.astype(jnp.float32) + projected).astype(jnp.bfloat16)
    updated_f32 = updated.astype(jnp.float32)
    inv_rms = lax.rsqrt(lax.optimization_barrier(jnp.mean(updated_f32 * updated_f32, axis=-1, keepdims=True)) + epsilon)
    normed = (updated_f32 * inv_rms * norm_gain).astype(jnp.bfloat16)
    shared_pre = jnp.dot(normed, shared_gate, preferred_element_type=jnp.float32)
    shared_lin = jnp.dot(normed, shared_up, preferred_element_type=jnp.float32)
    shared_act = (jax.nn.silu(shared_pre) * shared_lin).astype(jnp.bfloat16)
    shared_out = jnp.dot(shared_act, shared_down, preferred_element_type=jnp.float32)
    slot_dest = jax.vmap(block_slots)(routes.reshape(N_SP, TOK, TOPK))
    block_ids = jnp.broadcast_to(jnp.arange(N_SP, dtype=jnp.int32)[:, None], slot_dest.shape)
    token_ids = block_ids * TOK + (jnp.arange(TOK * TOPK, dtype=jnp.int32) // TOPK)[None, :]
    slot_token = jnp.full((N_SP, EXPERTS * CAP), -1, jnp.int32).at[block_ids, slot_dest].set(token_ids)
    slot_weight = jnp.zeros((N_SP, EXPERTS * CAP), jnp.float32).at[block_ids, slot_dest].set(route_weight.reshape(N_SP, TOK * TOPK))
    per_token = slot_token.reshape(N_SP, EXPERTS, CAP).transpose(1, 0, 2).reshape(EXPERTS, N_SP * CAP)
    per_weight = slot_weight.reshape(N_SP, EXPERTS, CAP).transpose(1, 0, 2).reshape(EXPERTS, N_SP * CAP)

    def one_expert(accum, inputs):
        gate_mat, up_mat, down_mat, token_list, weight_list = inputs
        filled = token_list >= 0
        safe_token = jnp.where(filled, token_list, 0).astype(jnp.int32)
        rows_in = jnp.where(filled[:, None], normed[safe_token], jnp.zeros((), jnp.bfloat16))
        gate_pre = jnp.dot(rows_in, gate_mat, preferred_element_type=jnp.float32)
        up_lin = jnp.dot(rows_in, up_mat, preferred_element_type=jnp.float32)
        expert_act = (jax.nn.silu(gate_pre) * up_lin).astype(jnp.bfloat16)
        expert_out = jnp.dot(expert_act, down_mat, preferred_element_type=jnp.float32).astype(jnp.bfloat16)
        accum = accum.at[safe_token].add(expert_out.astype(jnp.float32) * weight_list[:, None])
        return (accum, None)
    routed, _ = lax.scan(one_expert, jnp.zeros((TOKENS, D), jnp.float32), (expert_gate, expert_up, expert_down, per_token, per_weight))
    return (updated_f32 + shared_out + routed).astype(jnp.bfloat16)
```

```python
import functools

import jax
import jax.numpy as jnp
from jax import lax
from jax.experimental import pallas as pl
from jax.experimental.pallas import tpu as pltpu
from jax.sharding import PartitionSpec as P

HEAD_DIM = 64
WINDOW = 128
CORES = 2
GRP_SP = ("grp", "sp")
EPSILON = 1e-06
MESH = pl.DeviceIdType.MESH
BF16 = jnp.bfloat16
F32 = jnp.float32


def delta_order(nz):
    far = sorted((d if d <= nz // 2 else d - nz for d in range(nz)), key=lambda d: (-abs(d), -d))
    first = [d for d in far if abs(d) == nz // 4]
    return first + [d for d in far if d not in first]


class Ring:
    def __init__(self, n, me, buf, send_sem, recv_sem):
        self.n, self.me, self.buf, self.send_sem, self.recv_sem = n, me, buf, send_sem, recv_sem

    def hops(self, turn, right):
        longer = self.n // 2
        return longer if right == (turn % 2 == 0) else self.n - 1 - longer

    def copy(self, rows, index, right, hop):
        step = 1 if right else -1
        origin = lax.rem(self.me - step * (hop - 1) + self.n, self.n)
        target = lax.rem(self.me + step + self.n, self.n)
        ref = self.buf.at[origin, rows]
        return pltpu.make_async_remote_copy(
            src_ref=ref,
            dst_ref=ref,
            send_sem=self.send_sem,
            recv_sem=self.recv_sem.at[index, 0 if right else 1, hop - 1],
            device_id={"tp": target},
            device_id_type=MESH,
        )

    def arrival(self, rows, index, right, hop):
        step = 1 if right else -1
        origin = lax.rem(self.me - step * hop + self.n, self.n)
        ref = self.buf.at[origin, rows]
        pltpu.make_async_remote_copy(
            src_ref=ref,
            dst_ref=ref,
            send_sem=self.send_sem,
            recv_sem=self.recv_sem.at[index, 0 if right else 1, hop - 1],
            device_id={"tp": self.me},
            device_id_type=MESH,
        ).wait_recv()

    def begin(self, rows, index):
        for right in (True, False):
            if self.hops(index, right) > 0:
                self.copy(rows, index, right, 1).start()

    def pass_on(self, rows, index, hop):
        for right in (True, False):
            most = self.hops(index, right)
            if hop <= most:
                self.arrival(rows, index, right, hop)
                if hop < most:
                    self.copy(rows, index, right, hop + 1).start()

    def longest(self):
        return self.n // 2

    def finish(self):
        ref = self.buf.at[pl.ds(0, self.n - 1)]
        pltpu.make_async_remote_copy(
            src_ref=ref,
            dst_ref=ref,
            send_sem=self.send_sem,
            recv_sem=self.recv_sem.at[0, 0, 0],
            device_id={"tp": self.me},
            device_id_type=MESH,
        ).wait_send()


def layer(
    nsp,
    ntp,
    cap,
    residual,
    queries,
    keys,
    values,
    meta,
    sinks,
    out_weight,
    gain,
    expert_gate,
    expert_up,
    expert_down,
    shared_gate,
    shared_up,
    shared_down,
    out,
    halo_k,
    halo_v,
    halo_m,
    proj_w,
    res,
    att,
    upd,
    normed,
    scatter,
    pick,
    outgoing,
    rows_all,
    act_all,
    made,
    back,
    expert_in,
    expert_out,
    shared_in,
    shared_out,
    halo_send,
    halo_recv,
    w_send,
    w_recv,
    pair_send,
    pair_recv,
    att_send,
    att_recv,
    upd_send,
    upd_recv,
    disp_send,
    disp_recv,
    rows_send,
    rows_recv,
    act_send,
    act_recv,
    ret_send,
    ret_recv,
    load_sem,
):
    me = lax.axis_index("sp")
    tp = lax.axis_index("tp")
    nz = nsp // CORES
    z, core = me // CORES, lax.rem(me, CORES)
    tokens = queries.shape[0]
    cols = res.shape[1]
    heads_wide = queries.shape[1]
    blocks = tokens // WINDOW
    slots = nsp * cap
    hidden = expert_gate.shape[2]
    sibling = z * CORES + lax.rem(core + 1, CORES)
    following = lax.rem(me + 1, nsp)

    col_start = pl.multiple_of(tp * cols, cols)
    loads = [
        (residual.at[:, pl.ds(col_start, cols)], res),
        (shared_gate, shared_in.at[:, pl.ds(0, hidden)]),
        (shared_up, shared_in.at[:, pl.ds(hidden, hidden)]),
        (expert_gate.at[0], expert_in.at[:, pl.ds(0, hidden)]),
        (expert_up.at[0], expert_in.at[:, pl.ds(hidden, hidden)]),
        (expert_down.at[0], expert_out),
        (shared_down, shared_out),
    ]
    loads = [pltpu.make_async_copy(src, dst, load_sem.at[i]) for i, (src, dst) in enumerate(loads)]
    for load in loads:
        load.start()

    barrier = pltpu.get_barrier_semaphore()
    for d in range(1, nsp):
        pl.semaphore_signal(
            barrier, inc=1, device_id={"sp": lax.rem(me + d, nsp)}, device_id_type=MESH
        )
    for d in range(1, ntp):
        pl.semaphore_signal(
            barrier, inc=1, device_id={"tp": lax.rem(tp + d, ntp)}, device_id_type=MESH
        )
    pl.semaphore_wait(barrier, nsp - 1 + ntp - 1)

    tail = pl.ds(tokens - WINDOW, WINDOW)
    halo = [
        pltpu.make_async_remote_copy(
            src_ref=src,
            dst_ref=dst,
            send_sem=halo_send.at[i],
            recv_sem=halo_recv.at[i],
            device_id={"sp": following},
            device_id_type=MESH,
        )
        for i, (src, dst) in enumerate(
            [(keys.at[tail], halo_k), (values.at[tail], halo_v), (meta.at[:, tail], halo_m)]
        )
    ]
    for copy in halo:
        copy.start()

    part = heads_wide // CORES

    def weight_copy(d):
        target = lax.rem(tp + d, ntp)
        return pltpu.make_async_remote_copy(
            src_ref=out_weight.at[
                pl.ds(pl.multiple_of(core * part, part), part),
                pl.ds(pl.multiple_of(target * cols, cols), cols),
            ],
            dst_ref=proj_w.at[pl.ds(pl.multiple_of(tp * heads_wide + core * part, part), part)],
            send_sem=w_send.at[d - 1],
            recv_sem=w_recv.at[d - 1],
            device_id={"tp": target},
            device_id_type=MESH,
        )

    def weight_rows(d, which):
        source = lax.rem(tp - d + ntp, ntp)
        return proj_w.at[pl.ds(pl.multiple_of(source * heads_wide + which * part, part), part)]

    def pair_copy(d):
        ref = weight_rows(d, core)
        return pltpu.make_async_remote_copy(
            src_ref=ref,
            dst_ref=ref,
            send_sem=pair_send.at[d - 1],
            recv_sem=pair_recv.at[d - 1],
            device_id={"sp": sibling},
            device_id_type=MESH,
        )

    distances = sorted(range(1, ntp), key=lambda d: min(d, ntp - d))
    for d in distances:
        weight_copy(d).start()
    proj_w[pl.ds(pl.multiple_of(tp * heads_wide, heads_wide), heads_wide), :] = out_weight[
        :, pl.ds(col_start, cols)
    ]

    att_ring = Ring(ntp, tp, att, att_send, att_recv)
    upd_ring = Ring(ntp, tp, upd, upd_send, upd_recv)
    row_meta = meta[...]
    col_meta = jnp.transpose(row_meta)
    q_pos = lax.broadcasted_iota(jnp.int32, (WINDOW, 2 * WINDOW), 0)
    k_pos = lax.broadcasted_iota(jnp.int32, (WINDOW, 2 * WINDOW), 1)
    offset = q_pos + WINDOW - k_pos
    band = (offset >= 0) & (offset < WINDOW)

    def attend(b, band_k, band_v, band_seg):
        rows = slice(b * WINDOW, (b + 1) * WINDOW)
        allowed = band & (col_meta[rows, 0:1] == band_seg)
        heads = []
        for h in range(heads_wide // HEAD_DIM):
            q = queries[rows, h * HEAD_DIM : (h + 1) * HEAD_DIM]
            scores = lax.dot_general(
                q, band_k, (((1,), (1,)), ((), ())), preferred_element_type=F32
            ) * HEAD_DIM ** (-0.5)
            masked = jnp.where(allowed, scores, -jnp.inf)
            sink = sinks[h]
            top = jnp.maximum(jnp.max(masked, axis=-1, keepdims=True), sink)
            terms = jnp.exp(masked - top)
            denominator = jnp.sum(terms, axis=-1, keepdims=True) + jnp.exp(sink - top)
            weights = (terms / denominator).astype(BF16)
            heads.append(jnp.dot(weights, band_v, preferred_element_type=F32).astype(BF16))
        att[tp, rows, :] = jnp.concatenate(heads, axis=1)

    order = list(range(1, blocks)) + [0]
    span = [pl.ds(b * WINDOW, WINDOW) for b in range(blocks)]
    for b in order[:-1]:
        reach = slice((b - 1) * WINDOW, (b + 1) * WINDOW)
        attend(b, keys[reach, :], values[reach, :], row_meta[0:1, reach])
        att_ring.begin(span[b], b)
    for copy in halo:
        copy.wait_recv()
    halo_seg = jnp.where(me == 0, -1.0, halo_m[0:1, :])
    attend(
        0,
        jnp.concatenate([halo_k[...], keys[0:WINDOW, :]], axis=0),
        jnp.concatenate([halo_v[...], values[0:WINDOW, :]], axis=0),
        jnp.concatenate([halo_seg, row_meta[0:1, 0:WINDOW]], axis=1),
    )
    att_ring.begin(span[0], 0)

    route_of = [row_meta[1 + k : 2 + k, :] for k in range(2)]
    experts = lax.broadcasted_iota(jnp.int32, (nsp, tokens), 0).astype(F32)
    named = [(experts == r).astype(F32) for r in route_of]
    earlier = lax.broadcasted_iota(jnp.int32, (tokens, tokens), 0)
    later = lax.broadcasted_iota(jnp.int32, (tokens, tokens), 1)
    before = (earlier < later).astype(F32).astype(BF16)
    counts = jnp.dot((named[0] + named[1]).astype(BF16), before, preferred_element_type=F32)
    slot_row = [
        r * cap + jnp.sum(counts * m, axis=0, keepdims=True) for r, m in zip(route_of, named)
    ]
    slot_down = lax.broadcasted_iota(jnp.int32, (slots, tokens), 0).astype(F32)
    hit = (slot_down == slot_row[0]) | (slot_down == slot_row[1])
    scatter[...] = jnp.where(hit, 1.0, 0.0).astype(BF16)
    slot_col = jnp.transpose(
        jnp.concatenate([slot_row[0], slot_row[1], jnp.zeros((6, tokens), F32)], axis=0)
    )
    slot_along = lax.broadcasted_iota(jnp.int32, (tokens, slots), 1).astype(F32)
    for k in range(2):
        pick[k, :, :] = jnp.where(slot_along == slot_col[:, k : k + 1], 1.0, 0.0).astype(BF16)

    def weight_arrival(d):
        weight_copy(d).wait_recv()
        pair_copy(d).start()

    for hop in range(1, att_ring.longest() + 1):
        for b in order:
            att_ring.pass_on(span[b], b, hop)
        if hop == 1:
            for d in distances:
                weight_arrival(d)
    for d in distances:
        pair_copy(d).wait_recv()
    loads[0].wait()

    for b in order:
        rows = slice(b * WINDOW, (b + 1) * WINDOW)
        total = jnp.zeros((WINDOW, cols), F32)
        for s in range(ntp):
            total += jnp.dot(
                att[s, rows, :],
                proj_w[s * heads_wide : (s + 1) * heads_wide, :],
                preferred_element_type=F32,
            )
        upd[tp, rows, :] = (res[rows, :].astype(F32) + total).astype(BF16)
        upd_ring.begin(span[b], b)
    for hop in range(1, upd_ring.longest() + 1):
        for b in order:
            upd_ring.pass_on(span[b], b, hop)

    squares = jnp.zeros((tokens, 1), F32)
    for s in range(ntp):
        part_rows = upd[s].astype(F32)
        squares += jnp.sum(part_rows * part_rows, axis=-1, keepdims=True)
    inv_rms = lax.rsqrt(squares / (ntp * cols) + EPSILON)
    for s in range(ntp):
        normed[s] = (upd[s].astype(F32) * inv_rms * gain[s : s + 1, :]).astype(BF16)

    deltas = delta_order(nz)
    places = [(d, s) for d in deltas for s in range(CORES)]
    outgoing[...] = jnp.dot(scatter[...], normed[tp], preferred_element_type=F32).astype(BF16)

    def at_chip(d, s):
        return lax.rem(z + d + nz, nz) * CORES + lax.rem(core + s, CORES)

    def slot_block(index):
        return pl.ds(pl.multiple_of(index * cap, cap), cap)

    def dispatch_copy(i):
        d, s = places[i]
        target = at_chip(-d, s)
        return pltpu.make_async_remote_copy(
            src_ref=outgoing.at[slot_block(target)],
            dst_ref=rows_all.at[tp, pl.ds(i * cap, cap)],
            send_sem=disp_send,
            recv_sem=disp_recv.at[i],
            device_id={"sp": target},
            device_id_type=MESH,
        )

    own_place = places.index((0, 0))
    for i in range(nsp):
        if i != own_place:
            dispatch_copy(i).start()
    rows_all[tp, own_place * cap : (own_place + 1) * cap, :] = outgoing[slot_block(me), :]

    act_ring = Ring(ntp, tp, act_all, act_send, act_recv)
    rows_ring = Ring(ntp, tp, rows_all, rows_send, rows_recv)

    def activate(gate_up):
        gate, up = gate_up[:, :hidden], gate_up[:, hidden:]
        return (gate / (1.0 + jnp.exp(-gate)) * up).astype(BF16)

    for load in loads[1:]:
        load.wait()
    total = jnp.zeros((tokens, 2 * hidden), F32)
    for s in range(ntp):
        total += jnp.dot(
            normed[s], shared_in[s * cols : (s + 1) * cols, :], preferred_element_type=F32
        )
    act_all[tp, slots : slots + tokens, :] = activate(total)
    chunk_places = 2 * CORES
    chunks = nsp // chunk_places
    chunk = chunk_places * cap
    shared_span = pl.ds(slots, tokens)
    act_ring.begin(shared_span, chunks)

    def ready(q):
        for i in range(q * chunk_places, (q + 1) * chunk_places):
            if i != own_place:
                dispatch_copy(i).wait_recv()
        rows_ring.begin(pl.ds(q * chunk, chunk), q)

    def rows_hop(q, hop):
        rows_ring.pass_on(pl.ds(q * chunk, chunk), q, hop)

    def hidden_units(q):
        rows = slice(q * chunk, (q + 1) * chunk)
        total = jnp.zeros((chunk, 2 * hidden), F32)
        for s in range(ntp):
            total += jnp.dot(
                rows_all[s, rows, :],
                expert_in[s * cols : (s + 1) * cols, :],
                preferred_element_type=F32,
            )
        act_all[tp, rows, :] = activate(total)
        act_ring.begin(pl.ds(q * chunk, chunk), q)

    def act_hop(q, hop):
        act_ring.pass_on(pl.ds(q * chunk, chunk), q, hop)

    def shared_hop(hop):
        act_ring.pass_on(shared_span, chunks, hop)

    def return_copy(i):
        d, s = places[i]
        target = at_chip(d, s)
        return pltpu.make_async_remote_copy(
            src_ref=made.at[pl.ds(i * cap, cap)],
            dst_ref=back.at[slot_block(me)],
            send_sem=ret_send,
            recv_sem=ret_recv.at[i],
            device_id={"sp": target},
            device_id_type=MESH,
        )

    def outputs(q):
        rows = slice(q * chunk, (q + 1) * chunk)
        total = jnp.zeros((chunk, cols), F32)
        for s in range(ntp):
            total += jnp.dot(
                act_all[s, rows, :],
                expert_out[s * hidden : (s + 1) * hidden, :],
                preferred_element_type=F32,
            )
        made[rows, :] = total.astype(BF16)
        for i in range(q * chunk_places, (q + 1) * chunk_places):
            if i == own_place:
                back[slot_block(me), :] = made[i * cap : (i + 1) * cap, :]
            else:
                return_copy(i).start()

    period, row_hop, act_hop_time = 7.3, 4.0, 3.2
    head = 4.0
    longest = rows_ring.longest()
    steps = []
    for hop in range(1, longest + 1):
        steps.append((hop * 4.0, functools.partial(shared_hop, hop)))
    for q in range(chunks):
        at = head + q * period
        steps.append((at, functools.partial(ready, q)))
        for hop in range(1, longest + 1):
            steps.append((at + hop * row_hop, functools.partial(rows_hop, q, hop)))
        at += longest * row_hop + 0.1
        steps.append((at, functools.partial(hidden_units, q)))
        for hop in range(1, longest + 1):
            steps.append((at + hop * act_hop_time, functools.partial(act_hop, q, hop)))
        at += longest * act_hop_time + 0.1
        steps.append((at, functools.partial(outputs, q)))
    for _, step in sorted(steps, key=lambda step: step[0]):
        step()

    total = upd[tp].astype(F32)
    for s in range(ntp):
        total += jnp.dot(
            act_all[s, slots : slots + tokens, :],
            shared_out[s * hidden : (s + 1) * hidden, :],
            preferred_element_type=F32,
        )
    for i in range(nsp):
        if i != own_place:
            d, s = places[i]
            source = at_chip(-d, s)
            ref = back.at[slot_block(source)]
            pltpu.make_async_remote_copy(
                src_ref=ref,
                dst_ref=ref,
                send_sem=ret_send,
                recv_sem=ret_recv.at[i],
                device_id={"sp": source},
                device_id_type=MESH,
            ).wait_recv()
    for k in range(2):
        picked = jnp.dot(pick[k], back[...], preferred_element_type=F32)
        total += picked * col_meta[:, 3 + k : 4 + k]
    out[...] = total.astype(BF16)

    for copy in halo:
        copy.wait_send()
    for d in distances:
        weight_copy(d).wait_send()
        pair_copy(d).wait_send()
    for ring in (att_ring, upd_ring, rows_ring, act_ring):
        ring.finish()
    most = pl.ds(0, (nsp - 1) * cap)
    for buffer, sem in ((outgoing, disp_send), (made, ret_send)):
        ref = buffer.at[most]
        pltpu.make_async_remote_copy(
            src_ref=ref,
            dst_ref=ref,
            send_sem=sem,
            recv_sem=ret_recv.at[0],
            device_id={"sp": me},
            device_id_type=MESH,
        ).wait_send()


def shards(
    nsp,
    ntp,
    residual,
    queries,
    keys,
    values,
    segments,
    routes,
    route_weight,
    sinks,
    out_weight,
    norm_gain,
    expert_gate,
    expert_up,
    expert_down,
    shared_gate,
    shared_up,
    shared_down,
):
    tokens, width = residual.shape
    cols = width // ntp
    hidden = expert_gate.shape[2]
    heads_wide = queries.shape[1]
    cap = 2 * tokens * routes.shape[1] // nsp
    slots = nsp * cap
    chunks = nsp // (2 * CORES)
    longest = ntp // 2
    meta = jnp.concatenate(
        [
            segments[None].astype(F32),
            routes.T.astype(F32),
            route_weight.T,
            jnp.zeros((3, tokens), F32),
        ],
        axis=0,
    )
    vmem = pl.BlockSpec(memory_space=pltpu.VMEM)
    smem = pl.BlockSpec(memory_space=pltpu.SMEM)
    anywhere = pl.BlockSpec(memory_space=pl.ANY)
    dma = pltpu.SemaphoreType.DMA
    return pl.pallas_call(
        functools.partial(layer, nsp, ntp, cap),
        out_shape=jax.ShapeDtypeStruct((tokens, cols), BF16),
        in_specs=[anywhere, vmem, vmem, vmem, vmem, smem, vmem, vmem] + [anywhere] * 6,
        out_specs=vmem,
        scratch_shapes=[
            pltpu.VMEM((WINDOW, keys.shape[1]), BF16),
            pltpu.VMEM((WINDOW, values.shape[1]), BF16),
            pltpu.VMEM((8, WINDOW), F32),
            pltpu.VMEM((ntp * heads_wide, cols), BF16),
            pltpu.VMEM((tokens, cols), BF16),
            pltpu.VMEM((ntp, tokens, heads_wide), BF16),
            pltpu.VMEM((ntp, tokens, cols), BF16),
            pltpu.VMEM((ntp, tokens, cols), BF16),
            pltpu.VMEM((slots, tokens), BF16),
            pltpu.VMEM((2, tokens, slots), BF16),
            pltpu.VMEM((slots, cols), BF16),
            pltpu.VMEM((ntp, slots, cols), BF16),
            pltpu.VMEM((ntp, slots + tokens, hidden), BF16),
            pltpu.VMEM((slots, cols), BF16),
            pltpu.VMEM((slots, cols), BF16),
            pltpu.VMEM((width, 2 * hidden), BF16),
            pltpu.VMEM((ntp * hidden, cols), BF16),
            pltpu.VMEM((width, 2 * hidden), BF16),
            pltpu.VMEM((ntp * hidden, cols), BF16),
            dma((3,)),
            dma((3,)),
            dma((ntp - 1,)),
            dma((ntp - 1,)),
            dma((ntp - 1,)),
            dma((ntp - 1,)),
            dma,
            dma((tokens // WINDOW, 2, longest)),
            dma,
            dma((tokens // WINDOW, 2, longest)),
            dma,
            dma((nsp,)),
            dma,
            dma((chunks, 2, longest)),
            dma,
            dma((chunks + 1, 2, longest)),
            dma,
            dma((nsp,)),
            dma((7,)),
        ],
        compiler_params=pltpu.CompilerParams(collective_id=0, has_side_effects=True),
        name="layer",
    )(
        residual,
        queries,
        keys,
        values,
        meta,
        sinks,
        out_weight,
        norm_gain.reshape(ntp, cols),
        expert_gate,
        expert_up,
        expert_down,
        shared_gate,
        shared_up,
        shared_down,
    )


def solution(mesh):
    in_specs = (
        P(GRP_SP, None),
        P(GRP_SP, "tp"),
        P(GRP_SP, "tp"),
        P(GRP_SP, "tp"),
        P(GRP_SP),
        P(GRP_SP, None),
        P(GRP_SP, None),
        P("tp"),
        P("tp", None),
        P(),
        P("sp", None, "tp"),
        P("sp", None, "tp"),
        P("sp", None, "tp"),
        P(None, "tp"),
        P(None, "tp"),
        P(None, "tp"),
    )
    return jax.shard_map(
        functools.partial(shards, mesh.shape["sp"], mesh.shape["tp"]),
        mesh=mesh,
        in_specs=in_specs,
        out_specs=P(GRP_SP, "tp"),
        check_vma=False,
    )
```

```python
import functools

import jax
import jax.numpy as jnp
from jax import lax
from jax.experimental import pallas as pl
from jax.experimental.pallas import tpu as pltpu
from jax.sharding import PartitionSpec as P

HEAD_DIM = 64
WINDOW = 128
CORES = 2
GRP_SP = ("grp", "sp")
EPSILON = 1e-06
MESH = pl.DeviceIdType.MESH
BF16 = jnp.bfloat16
F32 = jnp.float32


NEAR = 1


def source_order(nz):
    spread = [d if d <= nz // 2 else d - nz for d in range(nz)]
    far = sorted((d for d in spread if abs(d) > NEAR), key=lambda d: (-abs(d), -d))
    early = [d for d in far if d == 2] + [d for d in far if abs(d) == 4]
    far = early + [d for d in far if d not in early]
    sizes, left = [], len(far)
    for size in [1] + [2] * len(far):
        tail = 2 if left > 4 else 1
        size = min(size, left, tail)
        if size:
            sizes.append(size)
            left -= size
    near = sorted((d for d in spread if abs(d) <= NEAR), key=lambda d: -abs(d))
    return far, near, sizes


class Ring:
    def __init__(self, n, me, buf, send_sem, recv_sem):
        self.n, self.me, self.buf, self.send_sem, self.recv_sem = n, me, buf, send_sem, recv_sem

    def hops(self, turn, right):
        longer = self.n // 2
        return longer if right == (turn % 2 == 0) else self.n - 1 - longer

    def copy(self, rows, index, right, hop):
        step = 1 if right else -1
        origin = lax.rem(self.me - step * (hop - 1) + self.n, self.n)
        target = lax.rem(self.me + step + self.n, self.n)
        ref = self.buf.at[origin, rows]
        return pltpu.make_async_remote_copy(
            src_ref=ref,
            dst_ref=ref,
            send_sem=self.send_sem,
            recv_sem=self.recv_sem.at[index, 0 if right else 1, hop - 1],
            device_id={"tp": target},
            device_id_type=MESH,
        )

    def arrival(self, rows, index, right, hop):
        step = 1 if right else -1
        origin = lax.rem(self.me - step * hop + self.n, self.n)
        ref = self.buf.at[origin, rows]
        pltpu.make_async_remote_copy(
            src_ref=ref,
            dst_ref=ref,
            send_sem=self.send_sem,
            recv_sem=self.recv_sem.at[index, 0 if right else 1, hop - 1],
            device_id={"tp": self.me},
            device_id_type=MESH,
        ).wait_recv()

    def begin(self, rows, index):
        for right in (True, False):
            if self.hops(index, right) > 0:
                self.copy(rows, index, right, 1).start()

    def pass_on(self, rows, index, hop):
        for right in (True, False):
            most = self.hops(index, right)
            if hop <= most:
                self.arrival(rows, index, right, hop)
                if hop < most:
                    self.copy(rows, index, right, hop + 1).start()

    def longest(self):
        return self.n // 2

    def finish(self, rows):
        ref = self.buf.at[pl.ds(0, self.n - 1), pl.ds(0, rows)]
        pltpu.make_async_remote_copy(
            src_ref=ref,
            dst_ref=ref,
            send_sem=self.send_sem,
            recv_sem=self.recv_sem.at[0, 0, 0],
            device_id={"tp": self.me},
            device_id_type=MESH,
        ).wait_send()


def layer(
    nsp,
    ntp,
    cap,
    residual,
    queries,
    keys,
    values,
    segments,
    routes,
    route_weight,
    sinks,
    out_weight,
    gain,
    expert_gate,
    expert_up,
    expert_down,
    shared_gate,
    shared_up,
    shared_down,
    out,
    halo_k,
    halo_v,
    halo_m,
    proj_w,
    res,
    att,
    upd,
    normed,
    scatter,
    pick,
    outgoing,
    near_out,
    sums,
    rows_all,
    act_all,
    made,
    back,
    expert_in,
    expert_out,
    shared_in,
    shared_out,
    halo_send,
    halo_recv,
    w_send,
    w_recv,
    pair_send,
    pair_recv,
    att_send,
    att_recv,
    upd_send,
    upd_recv,
    sum_send,
    sum_recv,
    disp_send,
    near_send,
    disp_recv,
    rows_send,
    rows_recv,
    act_send,
    act_recv,
    ret_send,
    ret_recv,
    load_sem,
    known_sem,
):
    me = lax.axis_index("sp")
    tp = lax.axis_index("tp")
    nz = nsp // CORES
    z, core = me // CORES, lax.rem(me, CORES)
    tokens = queries.shape[0]
    cols = res.shape[1]
    heads_wide = queries.shape[1]
    blocks = tokens // WINDOW
    slots = nsp * cap
    hidden = expert_gate.shape[2]
    sibling = z * CORES + lax.rem(core + 1, CORES)
    following = lax.rem(me + 1, nsp)

    col_start = pl.multiple_of(tp * cols, cols)
    loads = [
        (residual.at[:, pl.ds(col_start, cols)], res),
        (shared_gate, shared_in.at[:, pl.ds(0, hidden)]),
        (shared_up, shared_in.at[:, pl.ds(hidden, hidden)]),
        (expert_gate.at[0], expert_in.at[:, pl.ds(0, hidden)]),
        (expert_up.at[0], expert_in.at[:, pl.ds(hidden, hidden)]),
        (expert_down.at[0], expert_out),
        (shared_down, shared_out),
    ]
    loads = [pltpu.make_async_copy(src, dst, load_sem.at[i]) for i, (src, dst) in enumerate(loads)]
    for load in loads:
        load.start()

    nearby = [1, 2, -1, -2]
    barrier = pltpu.get_barrier_semaphore()
    for d in nearby:
        pl.semaphore_signal(
            barrier, inc=1, device_id={"sp": lax.rem(me + d + nsp, nsp)}, device_id_type=MESH
        )
    for d in range(1, ntp):
        pl.semaphore_signal(
            barrier, inc=1, device_id={"tp": lax.rem(tp + d, ntp)}, device_id_type=MESH
        )
    pl.semaphore_wait(barrier, len(nearby) + ntp - 1)
    reaches = []
    while (2 << len(reaches)) < nsp // 2:
        reaches.append(2 << len(reaches))

    def tell(r):
        for d in (reaches[r], -reaches[r]):
            pl.semaphore_signal(
                known_sem.at[r],
                inc=1,
                device_id={"sp": lax.rem(me + d + nsp, nsp)},
                device_id_type=MESH,
            )

    def hear(r):
        pl.semaphore_wait(known_sem.at[r], 2)

    if reaches:
        tell(0)

    tail = pl.ds(tokens - WINDOW, WINDOW)
    halo = [
        pltpu.make_async_remote_copy(
            src_ref=src,
            dst_ref=dst,
            send_sem=halo_send.at[i],
            recv_sem=halo_recv.at[i],
            device_id={"sp": following},
            device_id_type=MESH,
        )
        for i, (src, dst) in enumerate(
            [(keys.at[:, tail], halo_k), (values.at[:, tail], halo_v), (segments.at[:, tail], halo_m)]
        )
    ]
    for copy in halo:
        copy.start()

    part = heads_wide // CORES

    def weight_copy(d):
        target = lax.rem(tp + d, ntp)
        return pltpu.make_async_remote_copy(
            src_ref=out_weight.at[
                pl.ds(pl.multiple_of(core * part, part), part),
                pl.ds(pl.multiple_of(target * cols, cols), cols),
            ],
            dst_ref=proj_w.at[pl.ds(pl.multiple_of(tp * heads_wide + core * part, part), part)],
            send_sem=w_send.at[d - 1],
            recv_sem=w_recv.at[d - 1],
            device_id={"tp": target},
            device_id_type=MESH,
        )

    def weight_rows(d, which):
        source = lax.rem(tp - d + ntp, ntp)
        return proj_w.at[pl.ds(pl.multiple_of(source * heads_wide + which * part, part), part)]

    def pair_copy(d):
        ref = weight_rows(d, core)
        return pltpu.make_async_remote_copy(
            src_ref=ref,
            dst_ref=ref,
            send_sem=pair_send.at[d - 1],
            recv_sem=pair_recv.at[d - 1],
            device_id={"sp": sibling},
            device_id_type=MESH,
        )

    distances = sorted(range(1, ntp), key=lambda d: min(d, ntp - d))
    split = len(distances) // 2
    for d in distances[split:]:
        weight_copy(d).start()
    proj_w[pl.ds(pl.multiple_of(tp * heads_wide, heads_wide), heads_wide), :] = out_weight[
        :, pl.ds(col_start, cols)
    ]

    att_ring = Ring(ntp, tp, att, att_send, att_recv)
    upd_ring = Ring(ntp, tp, upd, upd_send, upd_recv)
    seg_row = segments[...].astype(F32)
    weight_row = route_weight[...]
    col_meta = jnp.transpose(
        jnp.concatenate([seg_row, weight_row, jnp.zeros((5, tokens), F32)], axis=0)
    )
    q_pos = lax.broadcasted_iota(jnp.int32, (WINDOW, 2 * WINDOW), 0)
    k_pos = lax.broadcasted_iota(jnp.int32, (WINDOW, 2 * WINDOW), 1)
    offset = q_pos + WINDOW - k_pos
    band = (offset >= 0) & (offset < WINDOW)

    def attend(b, band_k, band_v, band_seg):
        rows = slice(b * WINDOW, (b + 1) * WINDOW)
        allowed = band & (col_meta[rows, 0:1] == band_seg)
        heads = []
        for h in range(heads_wide // HEAD_DIM):
            q = queries[rows, h * HEAD_DIM : (h + 1) * HEAD_DIM]
            scores = jnp.dot(q, band_k, preferred_element_type=F32) * HEAD_DIM ** (-0.5)
            masked = jnp.where(allowed, scores, -jnp.inf)
            sink = sinks[h]
            top = jnp.maximum(jnp.max(masked, axis=-1, keepdims=True), sink)
            terms = jnp.exp(masked - top)
            denominator = jnp.sum(terms, axis=-1, keepdims=True) + jnp.exp(sink - top)
            weights = (terms / denominator).astype(BF16)
            mixed = lax.dot_general(
                weights, band_v, (((1,), (1,)), ((), ())), preferred_element_type=F32
            )
            heads.append(mixed.astype(BF16))
        att[tp, rows, :] = jnp.concatenate(heads, axis=1)

    order = list(range(1, blocks)) + [0]
    span = [pl.ds(b * WINDOW, WINDOW) for b in range(blocks)]
    for b in order[:-1]:
        reach = slice((b - 1) * WINDOW, (b + 1) * WINDOW)
        attend(b, keys[:, reach], values[:, reach], seg_row[:, reach])
        att_ring.begin(span[b], b)
    for d in distances[:split]:
        weight_copy(d).start()
    if reaches:
        hear(0)
    if len(reaches) > 1:
        tell(1)
    for copy in halo:
        copy.wait_recv()
    first = slice(0, WINDOW)
    halo_seg = jnp.where(me == 0, -1.0, halo_m[...].astype(F32))
    attend(
        0,
        jnp.concatenate([halo_k[...], keys[:, first]], axis=1),
        jnp.concatenate([halo_v[...], values[:, first]], axis=1),
        jnp.concatenate([halo_seg, seg_row[:, first]], axis=1),
    )
    att_ring.begin(span[0], 0)

    route_of = [routes[k : k + 1, :].astype(F32) for k in range(2)]
    experts = lax.broadcasted_iota(jnp.int32, (nsp, tokens), 0).astype(F32)
    named = [(experts == r).astype(F32) for r in route_of]
    earlier = lax.broadcasted_iota(jnp.int32, (tokens, tokens), 0)
    later = lax.broadcasted_iota(jnp.int32, (tokens, tokens), 1)
    before = (earlier < later).astype(F32).astype(BF16)
    counts = jnp.dot((named[0] + named[1]).astype(BF16), before, preferred_element_type=F32)
    slot_row = [
        r * cap + jnp.sum(counts * m, axis=0, keepdims=True) for r, m in zip(route_of, named)
    ]
    slot_down = lax.broadcasted_iota(jnp.int32, (slots, tokens), 0).astype(F32)
    hit = (slot_down == slot_row[0]) | (slot_down == slot_row[1])
    scatter[...] = jnp.where(hit, 1.0, 0.0).astype(BF16)
    slot_col = jnp.transpose(
        jnp.concatenate([slot_row[0], slot_row[1], jnp.zeros((6, tokens), F32)], axis=0)
    )
    slot_along = lax.broadcasted_iota(jnp.int32, (tokens, slots), 1).astype(F32)
    for k in range(2):
        pick[k, :, :] = jnp.where(slot_along == slot_col[:, k : k + 1], 1.0, 0.0).astype(BF16)

    def weight_arrival(d):
        weight_copy(d).wait_recv()
        pair_copy(d).start()

    for hop in range(1, att_ring.longest() + 1):
        for b in order:
            att_ring.pass_on(span[b], b, hop)
        if hop == 1:
            for r in range(1, len(reaches)):
                hear(r)
                if r + 1 < len(reaches):
                    tell(r + 1)
        if hop == 2:
            for d in distances[split:] + distances[:split]:
                weight_arrival(d)
    for d in distances:
        pair_copy(d).wait_recv()
    loads[0].wait()

    for b in order:
        rows = slice(b * WINDOW, (b + 1) * WINDOW)
        total = jnp.zeros((WINDOW, cols), F32)
        for s in range(ntp):
            total += jnp.dot(
                att[s, rows, :],
                proj_w[s * heads_wide : (s + 1) * heads_wide, :],
                preferred_element_type=F32,
            )
        upd[tp, rows, :] = (res[rows, :].astype(F32) + total).astype(BF16)
    own_cols = upd[tp].astype(F32)
    squares = jnp.sum(own_cols * own_cols, axis=-1, keepdims=True)
    sums[tp] = jnp.transpose(jnp.broadcast_to(squares, (tokens, 128)))[0:8, :]

    def sum_copy(d):
        return pltpu.make_async_remote_copy(
            src_ref=sums.at[tp],
            dst_ref=sums.at[tp],
            send_sem=sum_send.at[d - 1],
            recv_sem=sum_recv.at[d - 1],
            device_id={"tp": lax.rem(tp + d, ntp)},
            device_id_type=MESH,
        )

    def sum_arrival(d):
        source = lax.rem(tp - d + ntp, ntp)
        pltpu.make_async_remote_copy(
            src_ref=sums.at[source],
            dst_ref=sums.at[source],
            send_sem=sum_send.at[d - 1],
            recv_sem=sum_recv.at[d - 1],
            device_id={"tp": source},
            device_id_type=MESH,
        ).wait_recv()

    for d in distances[::-1]:
        sum_copy(d).start()
    for b in order:
        upd_ring.begin(span[b], b)
    for d in range(1, ntp):
        sum_arrival(d)
    squares = sums[0]
    for s in range(1, ntp):
        squares += sums[s]
    inv_rms = jnp.transpose(lax.rsqrt(squares / (ntp * cols) + EPSILON))[:, 0:1]

    far, near, sizes = source_order(nz)
    places = [(d, s) for d in far + near for s in range(CORES)]
    far_count = len(far) * CORES
    own_gain = gain[0:1, pl.ds(col_start, cols)]
    own_normed = (own_cols * inv_rms * own_gain).astype(BF16)
    outgoing[...] = jnp.dot(scatter[...], own_normed, preferred_element_type=F32).astype(BF16)

    def at_chip(d, s):
        return lax.rem(z + d + nz, nz) * CORES + lax.rem(core + s, CORES)

    def slot_block(index):
        return pl.ds(pl.multiple_of(index * cap, cap), cap)

    def dispatch_copy(i):
        d, s = places[i]
        target = at_chip(-d, s)
        return pltpu.make_async_remote_copy(
            src_ref=outgoing.at[slot_block(target)],
            dst_ref=rows_all.at[tp, pl.ds(i * cap, cap)],
            send_sem=disp_send,
            recv_sem=disp_recv.at[i],
            device_id={"sp": target},
            device_id_type=MESH,
        )

    for i in range(far_count):
        dispatch_copy(i).start()
    own_place = places.index((0, 0))

    act_ring = Ring(ntp, tp, act_all, act_send, act_recv)
    rows_ring = Ring(ntp, tp, rows_all, rows_send, rows_recv)

    def activate(gate_up):
        gate, up = gate_up[:, :hidden], gate_up[:, hidden:]
        return (gate / (1.0 + jnp.exp(-gate)) * up).astype(BF16)

    starts = [sum(sizes[:q]) * CORES for q in range(len(sizes) + 1)]
    far_chunks = len(sizes)
    near_chunk, shared_chunk = far_chunks, far_chunks + 1

    def places_of(q):
        if q == near_chunk:
            return range(far_count, nsp)
        return range(starts[q], starts[q + 1])

    def rows_of(q):
        if q == shared_chunk:
            return slots, tokens
        return places_of(q)[0] * cap, len(places_of(q)) * cap

    def span_of(q):
        return pl.ds(*rows_of(q))

    def upd_hop(hop):
        for b in order:
            upd_ring.pass_on(span[b], b, hop)

    near_places = [i for i in range(far_count, nsp) if i != own_place] + [own_place]

    def near_copy(j):
        i = near_places[j]
        target = at_chip(-places[i][0], places[i][1])
        return pltpu.make_async_remote_copy(
            src_ref=near_out.at[:, pl.ds(j * cap, cap)],
            dst_ref=rows_all.at[:, pl.ds(i * cap, cap)],
            send_sem=near_send,
            recv_sem=disp_recv.at[i],
            device_id={"sp": target},
            device_id_type=MESH,
        )

    def near_rows():
        chosen = jnp.concatenate(
            [scatter[slot_block(at_chip(-places[i][0], places[i][1])), :] for i in near_places],
            axis=0,
        )
        for s in range(ntp):
            normed[s] = (
                upd[s].astype(F32) * inv_rms * gain[0:1, s * cols : (s + 1) * cols]
            ).astype(BF16)
            picked = jnp.dot(chosen, normed[s], preferred_element_type=F32).astype(BF16)
            sent = (len(near_places) - 1) * cap
            near_out[s, 0:sent, :] = picked[:sent]
            rows_all[s, own_place * cap : (own_place + 1) * cap, :] = picked[sent:]
        for j in range(len(near_places) - 1):
            near_copy(j).start()

    def shared_units():
        total = jnp.zeros((tokens, 2 * hidden), F32)
        for s in range(ntp):
            total += jnp.dot(
                normed[s], shared_in[s * cols : (s + 1) * cols, :], preferred_element_type=F32
            )
        act_all[tp, slots : slots + tokens, :] = activate(total)
        act_ring.begin(span_of(shared_chunk), shared_chunk)

    for load in loads[1:]:
        load.wait()

    def ready(q):
        for i in places_of(q):
            dispatch_copy(i).wait_recv()
        rows_ring.begin(span_of(q), q)

    def rows_hop(q, hop):
        rows_ring.pass_on(span_of(q), q, hop)

    def hidden_units(q):
        if q == near_chunk:
            for j in range(len(near_places) - 1):
                near_copy(j).wait_recv()
        start, count = rows_of(q)
        total = jnp.zeros((count, 2 * hidden), F32)
        for s in range(ntp):
            total += jnp.dot(
                rows_all[s, start : start + count, :],
                expert_in[s * cols : (s + 1) * cols, :],
                preferred_element_type=F32,
            )
        act_all[tp, start : start + count, :] = activate(total)
        act_ring.begin(span_of(q), q)

    def act_hop(q, hop):
        act_ring.pass_on(span_of(q), q, hop)

    def return_copy(i):
        d, s = places[i]
        target = at_chip(d, s)
        return pltpu.make_async_remote_copy(
            src_ref=made.at[pl.ds(i * cap, cap)],
            dst_ref=back.at[slot_block(me)],
            send_sem=ret_send,
            recv_sem=ret_recv.at[i],
            device_id={"sp": target},
            device_id_type=MESH,
        )

    def outputs(q):
        start, count = rows_of(q)
        total = jnp.zeros((count, cols), F32)
        for s in range(ntp):
            total += jnp.dot(
                act_all[s, start : start + count, :],
                expert_out[s * hidden : (s + 1) * hidden, :],
                preferred_element_type=F32,
            )
        made[start : start + count, :] = total.astype(BF16)
        for i in places_of(q):
            if i == own_place:
                back[slot_block(me), :] = made[i * cap : (i + 1) * cap, :]
            else:
                return_copy(i).start()

    row_hop, act_hop_time, upd_hop_time = 5.0, 5.0, 4.0
    per_distance = 3.7
    longest = rows_ring.longest()
    steps = []
    for hop in range(1, longest + 1):
        steps.append((hop * upd_hop_time, functools.partial(upd_hop, hop)))
    steps.append((longest * upd_hop_time + 0.1, functools.partial(near_rows)))

    def act_steps(at, q):
        for hop in range(1, longest + 1):
            steps.append((at + hop * act_hop_time, functools.partial(act_hop, q, hop)))
        at += longest * act_hop_time + 0.1
        if q != shared_chunk:
            steps.append((at, functools.partial(outputs, q)))

    at = 4.0
    for q in range(far_chunks):
        steps.append((at, functools.partial(ready, q)))
        for hop in range(1, longest + 1):
            steps.append((at + hop * row_hop, functools.partial(rows_hop, q, hop)))
        done = at + longest * row_hop + 0.1
        steps.append((done, functools.partial(hidden_units, q)))
        act_steps(done, q)
        if q + 1 < far_chunks:
            at += sizes[q] * per_distance
    at = max(at, longest * upd_hop_time) + 4.0
    steps.append((at, functools.partial(hidden_units, near_chunk)))
    act_steps(at, near_chunk)
    at += 4.0
    steps.append((at, functools.partial(shared_units)))
    act_steps(at, shared_chunk)
    for _, step in sorted(steps, key=lambda step: step[0]):
        step()

    total = upd[tp].astype(F32)
    for s in range(ntp):
        total += jnp.dot(
            act_all[s, slots : slots + tokens, :],
            shared_out[s * hidden : (s + 1) * hidden, :],
            preferred_element_type=F32,
        )
    for i in range(nsp):
        if i != own_place:
            d, s = places[i]
            source = at_chip(-d, s)
            ref = back.at[slot_block(source)]
            pltpu.make_async_remote_copy(
                src_ref=ref,
                dst_ref=ref,
                send_sem=ret_send,
                recv_sem=ret_recv.at[i],
                device_id={"sp": source},
                device_id_type=MESH,
            ).wait_recv()
    for k in range(2):
        picked = jnp.dot(pick[k], back[...], preferred_element_type=F32)
        total += picked * col_meta[:, 1 + k : 2 + k]
    out[...] = total.astype(BF16)

    for copy in halo:
        copy.wait_send()
    for d in distances:
        weight_copy(d).wait_send()
        pair_copy(d).wait_send()
    for d in range(1, ntp):
        sum_copy(d).wait_send()
    att_ring.finish(tokens)
    upd_ring.finish(tokens)
    rows_ring.finish(far_count * cap)
    act_ring.finish(slots + tokens)
    sent = [
        (outgoing.at[pl.ds(0, far_count * cap)], disp_send),
        (near_out, near_send),
        (made.at[pl.ds(0, (nsp - 1) * cap)], ret_send),
    ]
    for ref, sem in sent:
        pltpu.make_async_remote_copy(
            src_ref=ref,
            dst_ref=ref,
            send_sem=sem,
            recv_sem=ret_recv.at[0],
            device_id={"sp": me},
            device_id_type=MESH,
        ).wait_send()


def shards(
    nsp,
    ntp,
    residual,
    queries,
    keys,
    values,
    segments,
    routes,
    route_weight,
    sinks,
    out_weight,
    norm_gain,
    expert_gate,
    expert_up,
    expert_down,
    shared_gate,
    shared_up,
    shared_down,
):
    tokens, width = residual.shape
    cols = width // ntp
    hidden = expert_gate.shape[2]
    heads_wide = queries.shape[1]
    cap = 2 * tokens * routes.shape[1] // nsp
    slots = nsp * cap
    longest = ntp // 2
    far, near, sizes = source_order(nsp // CORES)
    rounds = max(1, (nsp // 4).bit_length() - 1)
    vmem = pl.BlockSpec(memory_space=pltpu.VMEM)
    smem = pl.BlockSpec(memory_space=pltpu.SMEM)
    anywhere = pl.BlockSpec(memory_space=pl.ANY)
    dma = pltpu.SemaphoreType.DMA
    return pl.pallas_call(
        functools.partial(layer, nsp, ntp, cap),
        out_shape=jax.ShapeDtypeStruct((tokens, cols), BF16),
        in_specs=[anywhere] + [vmem] * 6 + [smem, vmem, vmem] + [anywhere] * 6,
        out_specs=vmem,
        scratch_shapes=[
            pltpu.VMEM((keys.shape[1], WINDOW), BF16),
            pltpu.VMEM((values.shape[1], WINDOW), BF16),
            pltpu.VMEM((1, WINDOW), jnp.int32),
            pltpu.VMEM((ntp * heads_wide, cols), BF16),
            pltpu.VMEM((tokens, cols), BF16),
            pltpu.VMEM((ntp, tokens, heads_wide), BF16),
            pltpu.VMEM((ntp, tokens, cols), BF16),
            pltpu.VMEM((ntp, tokens, cols), BF16),
            pltpu.VMEM((slots, tokens), BF16),
            pltpu.VMEM((2, tokens, slots), BF16),
            pltpu.VMEM((slots, cols), BF16),
            pltpu.VMEM((ntp, (len(near) * CORES - 1) * cap, cols), BF16),
            pltpu.VMEM((ntp, 8, tokens), F32),
            pltpu.VMEM((ntp, slots, cols), BF16),
            pltpu.VMEM((ntp, slots + tokens, hidden), BF16),
            pltpu.VMEM((slots, cols), BF16),
            pltpu.VMEM((slots, cols), BF16),
            pltpu.VMEM((width, 2 * hidden), BF16),
            pltpu.VMEM((ntp * hidden, cols), BF16),
            pltpu.VMEM((width, 2 * hidden), BF16),
            pltpu.VMEM((ntp * hidden, cols), BF16),
            dma((3,)),
            dma((3,)),
            dma((ntp - 1,)),
            dma((ntp - 1,)),
            dma((ntp - 1,)),
            dma((ntp - 1,)),
            dma,
            dma((tokens // WINDOW, 2, longest)),
            dma,
            dma((tokens // WINDOW, 2, longest)),
            dma((ntp - 1,)),
            dma((ntp - 1,)),
            dma,
            dma,
            dma((nsp,)),
            dma,
            dma((len(sizes), 2, longest)),
            dma,
            dma((len(sizes) + 2, 2, longest)),
            dma,
            dma((nsp,)),
            dma((7,)),
            pltpu.SemaphoreType.REGULAR((rounds,)),
        ],
        compiler_params=pltpu.CompilerParams(collective_id=0, has_side_effects=True),
        name="layer",
    )(
        residual,
        queries,
        keys.T,
        values.T,
        segments.reshape(1, tokens),
        routes.T,
        route_weight.T,
        sinks,
        out_weight,
        norm_gain.reshape(1, width),
        expert_gate,
        expert_up,
        expert_down,
        shared_gate,
        shared_up,
        shared_down,
    )


def solution(mesh):
    in_specs = (
        P(GRP_SP, None),
        P(GRP_SP, "tp"),
        P(GRP_SP, "tp"),
        P(GRP_SP, "tp"),
        P(GRP_SP),
        P(GRP_SP, None),
        P(GRP_SP, None),
        P("tp"),
        P("tp", None),
        P(),
        P("sp", None, "tp"),
        P("sp", None, "tp"),
        P("sp", None, "tp"),
        P(None, "tp"),
        P(None, "tp"),
        P(None, "tp"),
    )
    return jax.shard_map(
        functools.partial(shards, mesh.shape["sp"], mesh.shape["tp"]),
        mesh=mesh,
        in_specs=in_specs,
        out_specs=P(GRP_SP, "tp"),
        check_vma=False,
    )
```

```python
import functools

import jax
import jax.numpy as jnp
from jax import lax
from jax.experimental import pallas as pl
from jax.experimental.pallas import tpu as pltpu
from jax.sharding import PartitionSpec as P

HEAD_DIM = 64
WINDOW = 128
CORES = 2
GRP_SP = ("grp", "sp")
EPSILON = 1e-06
MESH = pl.DeviceIdType.MESH
BF16 = jnp.bfloat16
F32 = jnp.float32


def send_order(nz):
    spread = [d if d <= nz // 2 else d - nz for d in range(nz)]
    by_reach = sorted(spread, key=lambda d: (abs(d), -d))
    order = []
    while by_reach:
        order.append(by_reach.pop(0))
        if by_reach:
            order.append(by_reach.pop(0))
        if by_reach:
            order.append(by_reach.pop())
    return order


class Ring:
    def __init__(self, n, me, buf, send_sem, recv_sem):
        self.n, self.me, self.buf, self.send_sem, self.recv_sem = n, me, buf, send_sem, recv_sem

    def hops(self, turn, right):
        longer = self.n // 2
        return longer if right == (turn % 2 == 0) else self.n - 1 - longer

    def copy(self, rows, index, right, hop):
        step = 1 if right else -1
        origin = lax.rem(self.me - step * (hop - 1) + self.n, self.n)
        target = lax.rem(self.me + step + self.n, self.n)
        ref = self.buf.at[origin, rows]
        return pltpu.make_async_remote_copy(
            src_ref=ref,
            dst_ref=ref,
            send_sem=self.send_sem,
            recv_sem=self.recv_sem.at[index, 0 if right else 1, hop - 1],
            device_id={"tp": target},
            device_id_type=MESH,
        )

    def arrival(self, rows, index, right, hop):
        step = 1 if right else -1
        origin = lax.rem(self.me - step * hop + self.n, self.n)
        ref = self.buf.at[origin, rows]
        pltpu.make_async_remote_copy(
            src_ref=ref,
            dst_ref=ref,
            send_sem=self.send_sem,
            recv_sem=self.recv_sem.at[index, 0 if right else 1, hop - 1],
            device_id={"tp": self.me},
            device_id_type=MESH,
        ).wait_recv()

    def begin(self, rows, index):
        for right in (True, False):
            if self.hops(index, right) > 0:
                self.copy(rows, index, right, 1).start()

    def pass_on(self, rows, index, hop):
        for right in (True, False):
            most = self.hops(index, right)
            if hop <= most:
                self.arrival(rows, index, right, hop)
                if hop < most:
                    self.copy(rows, index, right, hop + 1).start()

    def longest(self):
        return self.n // 2

    def finish(self, rows):
        ref = self.buf.at[pl.ds(0, self.n - 1), pl.ds(0, rows)]
        pltpu.make_async_remote_copy(
            src_ref=ref,
            dst_ref=ref,
            send_sem=self.send_sem,
            recv_sem=self.recv_sem.at[0, 0, 0],
            device_id={"tp": self.me},
            device_id_type=MESH,
        ).wait_send()


class Leaps(Ring):
    def copy(self, rows, index, right, hop):
        step = 1 if right else -1
        kept = 0 if hop <= 2 else 2
        origin = lax.rem(self.me - step * kept + self.n, self.n)
        target = lax.rem(self.me + step * (hop - kept) + self.n, self.n)
        ref = self.buf.at[origin, rows]
        return pltpu.make_async_remote_copy(
            src_ref=ref,
            dst_ref=ref,
            send_sem=self.send_sem,
            recv_sem=self.recv_sem.at[index, 0 if right else 1, hop - 1],
            device_id={"tp": target},
            device_id_type=MESH,
        )

    def begin(self, rows, index):
        for hop in (2, 1):
            for right in (True, False):
                if hop <= self.hops(index, right):
                    self.copy(rows, index, right, hop).start()

    def pass_on(self, rows, index, hop):
        for right in (True, False):
            most = self.hops(index, right)
            if hop <= most:
                self.arrival(rows, index, right, hop)
                if hop == 2:
                    for later in range(most, 2, -1):
                        self.copy(rows, index, right, later).start()


def layer(
    nsp,
    ntp,
    cap,
    residual,
    queries,
    keys,
    values,
    segments,
    routes,
    route_weight,
    sinks,
    out_weight,
    gain,
    expert_gate,
    expert_up,
    expert_down,
    shared_gate,
    shared_up,
    shared_down,
    out,
    halo_k,
    halo_v,
    halo_m,
    proj_w,
    res,
    att,
    upd,
    normed,
    scatter,
    pick,
    outgoing,
    sums,
    rows_all,
    act_all,
    made,
    back,
    expert_in,
    expert_out,
    shared_in,
    shared_out,
    halo_send,
    halo_recv,
    w_send,
    w_recv,
    pair_send,
    pair_recv,
    att_send,
    att_recv,
    upd_send,
    upd_recv,
    sum_send,
    sum_recv,
    disp_send,
    disp_recv,
    rows_send,
    rows_recv,
    act_send,
    act_recv,
    ret_send,
    ret_recv,
    load_sem,
    chain_sem,
    all_in,
):
    me = lax.axis_index("sp")
    tp = lax.axis_index("tp")
    nz = nsp // CORES
    z, core = me // CORES, lax.rem(me, CORES)
    tokens = queries.shape[0]
    cols = res.shape[1]
    heads_wide = queries.shape[1]
    blocks = tokens // WINDOW
    slots = nsp * cap
    hidden = expert_gate.shape[2]
    sibling = z * CORES + lax.rem(core + 1, CORES)
    following = lax.rem(me + 1, nsp)

    col_start = pl.multiple_of(tp * cols, cols)
    loads = [
        (residual.at[:, pl.ds(col_start, cols)], res),
        (shared_gate, shared_in.at[:, pl.ds(0, hidden)]),
        (shared_up, shared_in.at[:, pl.ds(hidden, hidden)]),
        (expert_gate.at[0], expert_in.at[:, pl.ds(0, hidden)]),
        (expert_up.at[0], expert_in.at[:, pl.ds(hidden, hidden)]),
        (expert_down.at[0], expert_out),
        (shared_down, shared_out),
    ]
    loads = [pltpu.make_async_copy(src, dst, load_sem.at[i]) for i, (src, dst) in enumerate(loads)]
    for load in loads:
        load.start()

    def say(semaphore, where):
        pl.semaphore_signal(semaphore, inc=1, device_id=where, device_id_type=MESH)

    last = (me + 1) // nsp
    barrier = pltpu.get_barrier_semaphore()
    for d in range(1, ntp):
        say(barrier, {"tp": lax.rem(tp + d, ntp)})
    say(barrier, {"sp": sibling})

    @pl.when(core == 0)
    def _():
        say(barrier, {"sp": lax.rem(me + nsp - 1, nsp)})

    @pl.when(me == 1)
    def _():
        say(barrier, {"sp": nsp - 1})

    pl.semaphore_wait(barrier, ntp + core + last)

    @pl.when(me >= 3)
    def _():
        pl.semaphore_wait(chain_sem, 1)

    @pl.when((me >= 2) & (me < nsp - 1))
    def _():
        say(chain_sem, {"sp": following})

    @pl.when(me == nsp - 1)
    def _():
        for j in range(nsp - 1):
            say(all_in, {"sp": j})

    tail = pl.ds(tokens - WINDOW, WINDOW)
    halo = [
        pltpu.make_async_remote_copy(
            src_ref=src,
            dst_ref=dst,
            send_sem=halo_send.at[i],
            recv_sem=halo_recv.at[i],
            device_id={"sp": following},
            device_id_type=MESH,
        )
        for i, (src, dst) in enumerate(
            [(keys.at[:, tail], halo_k), (values.at[:, tail], halo_v), (segments.at[:, tail], halo_m)]
        )
    ]

    @pl.when(me < nsp - 1)
    def _():
        for copy in halo:
            copy.start()


    part = heads_wide // CORES

    def weight_copy(d):
        target = lax.rem(tp + d, ntp)
        return pltpu.make_async_remote_copy(
            src_ref=out_weight.at[
                pl.ds(pl.multiple_of(core * part, part), part),
                pl.ds(pl.multiple_of(target * cols, cols), cols),
            ],
            dst_ref=proj_w.at[pl.ds(pl.multiple_of(tp * heads_wide + core * part, part), part)],
            send_sem=w_send.at[d - 1],
            recv_sem=w_recv.at[d - 1],
            device_id={"tp": target},
            device_id_type=MESH,
        )

    def weight_rows(d, which):
        source = lax.rem(tp - d + ntp, ntp)
        return proj_w.at[pl.ds(pl.multiple_of(source * heads_wide + which * part, part), part)]

    def pair_copy(d):
        ref = weight_rows(d, core)
        return pltpu.make_async_remote_copy(
            src_ref=ref,
            dst_ref=ref,
            send_sem=pair_send.at[d - 1],
            recv_sem=pair_recv.at[d - 1],
            device_id={"sp": sibling},
            device_id_type=MESH,
        )

    distances = sorted(range(1, ntp), key=lambda d: min(d, ntp - d))
    split = len(distances) // 2
    for d in distances[split:]:
        weight_copy(d).start()
    proj_w[pl.ds(pl.multiple_of(tp * heads_wide, heads_wide), heads_wide), :] = out_weight[
        :, pl.ds(col_start, cols)
    ]

    att_ring = Leaps(ntp, tp, att, att_send, att_recv)
    upd_ring = Ring(ntp, tp, upd, upd_send, upd_recv)
    seg_row = segments[...].astype(F32)
    weight_row = route_weight[...]
    col_meta = jnp.transpose(
        jnp.concatenate([seg_row, weight_row, jnp.zeros((5, tokens), F32)], axis=0)
    )
    q_pos = lax.broadcasted_iota(jnp.int32, (WINDOW, 2 * WINDOW), 0)
    k_pos = lax.broadcasted_iota(jnp.int32, (WINDOW, 2 * WINDOW), 1)
    offset = q_pos + WINDOW - k_pos
    band = (offset >= 0) & (offset < WINDOW)

    def attend(b, band_k, band_v, band_seg):
        rows = slice(b * WINDOW, (b + 1) * WINDOW)
        allowed = band & (col_meta[rows, 0:1] == band_seg)
        heads = []
        for h in range(heads_wide // HEAD_DIM):
            q = queries[rows, h * HEAD_DIM : (h + 1) * HEAD_DIM]
            scores = jnp.dot(q, band_k, preferred_element_type=F32) * HEAD_DIM ** (-0.5)
            masked = jnp.where(allowed, scores, -jnp.inf)
            sink = sinks[h]
            top = jnp.maximum(jnp.max(masked, axis=-1, keepdims=True), sink)
            terms = jnp.exp(masked - top)
            denominator = jnp.sum(terms, axis=-1, keepdims=True) + jnp.exp(sink - top)
            weights = (terms / denominator).astype(BF16)
            mixed = lax.dot_general(
                weights, band_v, (((1,), (1,)), ((), ())), preferred_element_type=F32
            )
            heads.append(mixed.astype(BF16))
        att[tp, rows, :] = jnp.concatenate(heads, axis=1)

    order = list(range(1, blocks)) + [0]
    span = [pl.ds(b * WINDOW, WINDOW) for b in range(blocks)]
    for b in order[:-1]:
        reach = slice((b - 1) * WINDOW, (b + 1) * WINDOW)
        attend(b, keys[:, reach], values[:, reach], seg_row[:, reach])
        att_ring.begin(span[b], b)
    for d in distances[:split]:
        weight_copy(d).start()

    @pl.when(me > 0)
    def _():
        for copy in halo:
            copy.wait_recv()

    @pl.when(me == 0)
    def _():
        for ref in (halo_k, halo_v, halo_m):
            ref[...] = jnp.zeros_like(ref)

    first = slice(0, WINDOW)
    halo_seg = jnp.where(me == 0, -1.0, halo_m[...].astype(F32))
    attend(
        0,
        jnp.concatenate([halo_k[...], keys[:, first]], axis=1),
        jnp.concatenate([halo_v[...], values[:, first]], axis=1),
        jnp.concatenate([halo_seg, seg_row[:, first]], axis=1),
    )
    att_ring.begin(span[0], 0)

    route_of = [routes[k : k + 1, :].astype(F32) for k in range(2)]
    experts = lax.broadcasted_iota(jnp.int32, (nsp, tokens), 0).astype(F32)
    named = [(experts == r).astype(F32) for r in route_of]
    earlier = lax.broadcasted_iota(jnp.int32, (tokens, tokens), 0)
    later = lax.broadcasted_iota(jnp.int32, (tokens, tokens), 1)
    before = (earlier < later).astype(F32).astype(BF16)
    counts = jnp.dot((named[0] + named[1]).astype(BF16), before, preferred_element_type=F32)
    slot_row = [
        r * cap + jnp.sum(counts * m, axis=0, keepdims=True) for r, m in zip(route_of, named)
    ]
    slot_down = lax.broadcasted_iota(jnp.int32, (slots, tokens), 0).astype(F32)
    hit = (slot_down == slot_row[0]) | (slot_down == slot_row[1])
    scatter[...] = jnp.where(hit, 1.0, 0.0).astype(BF16)
    slot_col = jnp.transpose(
        jnp.concatenate([slot_row[0], slot_row[1], jnp.zeros((6, tokens), F32)], axis=0)
    )
    slot_along = lax.broadcasted_iota(jnp.int32, (tokens, slots), 1).astype(F32)
    for k in range(2):
        pick[k, :, :] = jnp.where(slot_along == slot_col[:, k : k + 1], 1.0, 0.0).astype(BF16)

    def weight_arrival(d):
        weight_copy(d).wait_recv()
        pair_copy(d).start()

    hops = list(range(1, att_ring.longest() + 1))
    for hop in hops[1:2] + hops[:1] + hops[2:]:
        for b in order:
            att_ring.pass_on(span[b], b, hop)
        if hop == 1:
            for d in distances[split:] + distances[:split]:
                weight_arrival(d)
    for d in distances:
        pair_copy(d).wait_recv()
    loads[0].wait()

    for b in order:
        rows = slice(b * WINDOW, (b + 1) * WINDOW)
        total = jnp.zeros((WINDOW, cols), F32)
        for s in range(ntp):
            total += jnp.dot(
                att[s, rows, :],
                proj_w[s * heads_wide : (s + 1) * heads_wide, :],
                preferred_element_type=F32,
            )
        upd[tp, rows, :] = (res[rows, :].astype(F32) + total).astype(BF16)
    own_cols = upd[tp].astype(F32)
    squares = jnp.sum(own_cols * own_cols, axis=-1, keepdims=True)
    sums[tp] = jnp.transpose(jnp.broadcast_to(squares, (tokens, 128)))[0:8, :]

    def sum_copy(d):
        return pltpu.make_async_remote_copy(
            src_ref=sums.at[tp],
            dst_ref=sums.at[tp],
            send_sem=sum_send.at[d - 1],
            recv_sem=sum_recv.at[d - 1],
            device_id={"tp": lax.rem(tp + d, ntp)},
            device_id_type=MESH,
        )

    def sum_arrival(d):
        source = lax.rem(tp - d + ntp, ntp)
        pltpu.make_async_remote_copy(
            src_ref=sums.at[source],
            dst_ref=sums.at[source],
            send_sem=sum_send.at[d - 1],
            recv_sem=sum_recv.at[d - 1],
            device_id={"tp": source},
            device_id_type=MESH,
        ).wait_recv()

    for d in distances[::-1]:
        sum_copy(d).start()
    for b in order:
        upd_ring.begin(span[b], b)
    for d in range(1, ntp):
        sum_arrival(d)
    squares = sums[0]
    for s in range(1, ntp):
        squares += sums[s]
    inv_rms = jnp.transpose(lax.rsqrt(squares / (ntp * cols) + EPSILON))[:, 0:1]

    chips = send_order(nz)
    places = [(d, s) for d in chips for s in range(CORES) if (d, s) != (0, 0)]
    own_gain = gain[0:1, pl.ds(col_start, cols)]
    own_normed = (own_cols * inv_rms * own_gain).astype(BF16)
    outgoing[...] = jnp.dot(scatter[...], own_normed, preferred_element_type=F32).astype(BF16)

    def at_chip(d, s):
        return lax.rem(z + d + nz, nz) * CORES + lax.rem(core + s, CORES)

    def slot_block(index):
        return pl.ds(pl.multiple_of(index * cap, cap), cap)

    def dispatch_copy(i):
        d, s = places[i]
        target = at_chip(d, s)
        return pltpu.make_async_remote_copy(
            src_ref=outgoing.at[slot_block(target)],
            dst_ref=rows_all.at[tp, slot_block(me)],
            send_sem=disp_send,
            recv_sem=disp_recv.at[me],
            device_id={"sp": target},
            device_id_type=MESH,
        )

    rows_all[tp, slot_block(me), :] = outgoing[slot_block(me), :]

    @pl.when(me < nsp - 1)
    def _():
        pl.semaphore_wait(all_in, 1)

    for i in range(len(places)):
        dispatch_copy(i).start()

    def block_wait(ref, sem):
        pltpu.make_async_remote_copy(
            src_ref=ref,
            dst_ref=ref,
            send_sem=disp_send,
            recv_sem=sem,
            device_id={"sp": me},
            device_id_type=MESH,
        ).wait_recv()

    act_ring = Ring(ntp, tp, act_all, act_send, act_recv)
    rows_ring = Ring(ntp, tp, rows_all, rows_send, rows_recv)

    def activate(gate_up):
        gate, up = gate_up[:, :hidden], gate_up[:, hidden:]
        return (gate / (1.0 + jnp.exp(-gate)) * up).astype(BF16)

    chunk_sources = 2 * CORES
    chunks = nsp // chunk_sources
    shared_chunk = chunks

    def places_of(q):
        return range(q * chunk_sources, (q + 1) * chunk_sources)

    def rows_of(q):
        if q == shared_chunk:
            return slots, tokens
        return q * chunk_sources * cap, chunk_sources * cap

    def span_of(q):
        return pl.ds(*rows_of(q))

    def upd_hop(hop):
        for b in order:
            upd_ring.pass_on(span[b], b, hop)

    def shared_units():
        total = jnp.zeros((tokens, 2 * hidden), F32)
        for s in range(ntp):
            normed[s] = (
                upd[s].astype(F32) * inv_rms * gain[0:1, s * cols : (s + 1) * cols]
            ).astype(BF16)
            total += jnp.dot(
                normed[s], shared_in[s * cols : (s + 1) * cols, :], preferred_element_type=F32
            )
        act_all[tp, slots : slots + tokens, :] = activate(total)
        act_ring.begin(span_of(shared_chunk), shared_chunk)

    for load in loads[1:]:
        load.wait()

    def ready(q):
        for source in places_of(q):

            @pl.when(me != source)
            def _():
                block_wait(rows_all.at[tp, pl.ds(source * cap, cap)], disp_recv.at[source])

        rows_ring.begin(span_of(q), q)

    def rows_hop(q, hop):
        rows_ring.pass_on(span_of(q), q, hop)

    def hidden_units(q):
        start, count = rows_of(q)
        total = jnp.zeros((count, 2 * hidden), F32)
        for s in range(ntp):
            total += jnp.dot(
                rows_all[s, start : start + count, :],
                expert_in[s * cols : (s + 1) * cols, :],
                preferred_element_type=F32,
            )
        act_all[tp, start : start + count, :] = activate(total)
        act_ring.begin(span_of(q), q)

    def act_hop(q, hop):
        act_ring.pass_on(span_of(q), q, hop)

    def return_copy(source):
        return pltpu.make_async_remote_copy(
            src_ref=made.at[pl.ds(source * cap, cap)],
            dst_ref=back.at[slot_block(me)],
            send_sem=ret_send,
            recv_sem=ret_recv.at[me],
            device_id={"sp": source},
            device_id_type=MESH,
        )

    def outputs(q):
        start, count = rows_of(q)
        total = jnp.zeros((count, cols), F32)
        for s in range(ntp):
            total += jnp.dot(
                act_all[s, start : start + count, :],
                expert_out[s * hidden : (s + 1) * hidden, :],
                preferred_element_type=F32,
            )
        made[start : start + count, :] = total.astype(BF16)
        for source in places_of(q):

            @pl.when(me == source)
            def _():
                back[slot_block(me), :] = made[source * cap : (source + 1) * cap, :]

            @pl.when(me != source)
            def _():
                return_copy(source).start()

    row_hop, act_hop_time, upd_hop_time, period = 5.0, 5.0, 3.0, 7.4
    longest = rows_ring.longest()
    steps = []
    for hop in range(1, longest + 1):
        steps.append((hop * upd_hop_time, functools.partial(upd_hop, hop)))

    def act_steps(at, q):
        for hop in range(1, longest + 1):
            steps.append((at + hop * act_hop_time, functools.partial(act_hop, q, hop)))
        at += longest * act_hop_time + 0.1
        if q != shared_chunk:
            steps.append((at, functools.partial(outputs, q)))

    in_turn = list(range(1, min(3, chunks))) + [0] + list(range(3, chunks))
    at = 8.0
    for q in in_turn:
        steps.append((at, functools.partial(ready, q)))
        for hop in range(1, longest + 1):
            steps.append((at + hop * row_hop, functools.partial(rows_hop, q, hop)))
        done = at + longest * row_hop + 0.1
        steps.append((done, functools.partial(hidden_units, q)))
        act_steps(done, q)
        at += period
    at = max(at, longest * upd_hop_time) + 1.0
    steps.append((at, functools.partial(shared_units)))
    act_steps(at, shared_chunk)
    for _, step in sorted(steps, key=lambda step: step[0]):
        step()

    total = upd[tp].astype(F32)
    for s in range(ntp):
        total += jnp.dot(
            act_all[s, slots : slots + tokens, :],
            shared_out[s * hidden : (s + 1) * hidden, :],
            preferred_element_type=F32,
        )
    for expert in range(nsp):

        @pl.when(me != expert)
        def _():
            block_wait(back.at[pl.ds(expert * cap, cap)], ret_recv.at[expert])

    for k in range(2):
        picked = jnp.dot(pick[k], back[...], preferred_element_type=F32)
        total += picked * col_meta[:, 1 + k : 2 + k]
    out[...] = total.astype(BF16)

    @pl.when(me < nsp - 1)
    def _():
        for copy in halo:
            copy.wait_send()

    for d in distances:
        weight_copy(d).wait_send()
        pair_copy(d).wait_send()
    for d in range(1, ntp):
        sum_copy(d).wait_send()
    att_ring.finish(tokens)
    upd_ring.finish(tokens)
    rows_ring.finish(slots)
    act_ring.finish(slots + tokens)
    sent = [
        (outgoing.at[pl.ds(0, (nsp - 1) * cap)], disp_send),
        (made.at[pl.ds(0, (nsp - 1) * cap)], ret_send),
    ]
    for ref, sem in sent:
        pltpu.make_async_remote_copy(
            src_ref=ref,
            dst_ref=ref,
            send_sem=sem,
            recv_sem=ret_recv.at[0],
            device_id={"sp": me},
            device_id_type=MESH,
        ).wait_send()


def shards(
    nsp,
    ntp,
    residual,
    queries,
    keys,
    values,
    segments,
    routes,
    route_weight,
    sinks,
    out_weight,
    norm_gain,
    expert_gate,
    expert_up,
    expert_down,
    shared_gate,
    shared_up,
    shared_down,
):
    tokens, width = residual.shape
    cols = width // ntp
    hidden = expert_gate.shape[2]
    heads_wide = queries.shape[1]
    cap = 2 * tokens * routes.shape[1] // nsp
    slots = nsp * cap
    longest = ntp // 2
    chunks = nsp // (2 * CORES)
    vmem = pl.BlockSpec(memory_space=pltpu.VMEM)
    smem = pl.BlockSpec(memory_space=pltpu.SMEM)
    anywhere = pl.BlockSpec(memory_space=pl.ANY)
    dma = pltpu.SemaphoreType.DMA
    return pl.pallas_call(
        functools.partial(layer, nsp, ntp, cap),
        out_shape=jax.ShapeDtypeStruct((tokens, cols), BF16),
        in_specs=[anywhere] + [vmem] * 6 + [smem, vmem, vmem] + [anywhere] * 6,
        out_specs=vmem,
        scratch_shapes=[
            pltpu.VMEM((keys.shape[1], WINDOW), BF16),
            pltpu.VMEM((values.shape[1], WINDOW), BF16),
            pltpu.VMEM((1, WINDOW), jnp.int32),
            pltpu.VMEM((ntp * heads_wide, cols), BF16),
            pltpu.VMEM((tokens, cols), BF16),
            pltpu.VMEM((ntp, tokens, heads_wide), BF16),
            pltpu.VMEM((ntp, tokens, cols), BF16),
            pltpu.VMEM((ntp, tokens, cols), BF16),
            pltpu.VMEM((slots, tokens), BF16),
            pltpu.VMEM((2, tokens, slots), BF16),
            pltpu.VMEM((slots, cols), BF16),
            pltpu.VMEM((ntp, 8, tokens), F32),
            pltpu.VMEM((ntp, slots, cols), BF16),
            pltpu.VMEM((ntp, slots + tokens, hidden), BF16),
            pltpu.VMEM((slots, cols), BF16),
            pltpu.VMEM((slots, cols), BF16),
            pltpu.VMEM((width, 2 * hidden), BF16),
            pltpu.VMEM((ntp * hidden, cols), BF16),
            pltpu.VMEM((width, 2 * hidden), BF16),
            pltpu.VMEM((ntp * hidden, cols), BF16),
            dma((3,)),
            dma((3,)),
            dma((ntp - 1,)),
            dma((ntp - 1,)),
            dma((ntp - 1,)),
            dma((ntp - 1,)),
            dma,
            dma((tokens // WINDOW, 2, longest)),
            dma,
            dma((tokens // WINDOW, 2, longest)),
            dma((ntp - 1,)),
            dma((ntp - 1,)),
            dma,
            dma((nsp,)),
            dma,
            dma((chunks, 2, longest)),
            dma,
            dma((chunks + 1, 2, longest)),
            dma,
            dma((nsp,)),
            dma((7,)),
            pltpu.SemaphoreType.REGULAR,
            pltpu.SemaphoreType.REGULAR,
        ],
        compiler_params=pltpu.CompilerParams(collective_id=0, has_side_effects=True),
        name="layer",
    )(
        residual,
        queries,
        keys.T,
        values.T,
        segments.reshape(1, tokens),
        routes.T,
        route_weight.T,
        sinks,
        out_weight,
        norm_gain.reshape(1, width),
        expert_gate,
        expert_up,
        expert_down,
        shared_gate,
        shared_up,
        shared_down,
    )


def solution(mesh):
    in_specs = (
        P(GRP_SP, None),
        P(GRP_SP, "tp"),
        P(GRP_SP, "tp"),
        P(GRP_SP, "tp"),
        P(GRP_SP),
        P(GRP_SP, None),
        P(GRP_SP, None),
        P("tp"),
        P("tp", None),
        P(),
        P("sp", None, "tp"),
        P("sp", None, "tp"),
        P("sp", None, "tp"),
        P(None, "tp"),
        P(None, "tp"),
        P(None, "tp"),
    )
    return jax.shard_map(
        functools.partial(shards, mesh.shape["sp"], mesh.shape["tp"]),
        mesh=mesh,
        in_specs=in_specs,
        out_specs=P(GRP_SP, "tp"),
        check_vma=False,
    )
```

```python
import functools

import jax
import jax.numpy as jnp
from jax import lax
from jax.experimental import pallas as pl
from jax.experimental.pallas import tpu as pltpu
from jax.sharding import PartitionSpec as P

HEAD_DIM = 64
WINDOW = 128
CORES = 2
GRP_SP = ("grp", "sp")
EPSILON = 1e-06
MESH = pl.DeviceIdType.MESH
BF16 = jnp.bfloat16
F32 = jnp.float32


def send_order(nz):
    spread = [d if d <= nz // 2 else d - nz for d in range(nz)]
    by_reach = sorted(spread, key=lambda d: (abs(d), -d))
    order = []
    while by_reach:
        order.append(by_reach.pop(0))
        if by_reach:
            order.append(by_reach.pop(0))
        if by_reach:
            order.append(by_reach.pop())
    return order


class Ring:
    def __init__(self, n, me, buf, send_sem, recv_sem):
        self.n, self.me, self.buf, self.send_sem, self.recv_sem = n, me, buf, send_sem, recv_sem

    def hops(self, turn, right):
        longer = self.n // 2
        return longer if right == (turn % 2 == 0) else self.n - 1 - longer

    def copy(self, rows, index, right, hop):
        step = 1 if right else -1
        origin = lax.rem(self.me - step * (hop - 1) + self.n, self.n)
        target = lax.rem(self.me + step + self.n, self.n)
        ref = self.buf.at[origin, rows]
        return pltpu.make_async_remote_copy(
            src_ref=ref,
            dst_ref=ref,
            send_sem=self.send_sem,
            recv_sem=self.recv_sem.at[index, 0 if right else 1, hop - 1],
            device_id={"tp": target},
            device_id_type=MESH,
        )

    def arrival(self, rows, index, right, hop):
        step = 1 if right else -1
        origin = lax.rem(self.me - step * hop + self.n, self.n)
        ref = self.buf.at[origin, rows]
        pltpu.make_async_remote_copy(
            src_ref=ref,
            dst_ref=ref,
            send_sem=self.send_sem,
            recv_sem=self.recv_sem.at[index, 0 if right else 1, hop - 1],
            device_id={"tp": self.me},
            device_id_type=MESH,
        ).wait_recv()

    def begin(self, rows, index):
        for right in (True, False):
            if self.hops(index, right) > 0:
                self.copy(rows, index, right, 1).start()

    def pass_on(self, rows, index, hop):
        for right in (True, False):
            most = self.hops(index, right)
            if hop <= most:
                self.arrival(rows, index, right, hop)
                if hop < most:
                    self.copy(rows, index, right, hop + 1).start()

    def longest(self):
        return self.n // 2

    def finish(self, rows):
        ref = self.buf.at[pl.ds(0, self.n - 1), pl.ds(0, rows)]
        pltpu.make_async_remote_copy(
            src_ref=ref,
            dst_ref=ref,
            send_sem=self.send_sem,
            recv_sem=self.recv_sem.at[0, 0, 0],
            device_id={"tp": self.me},
            device_id_type=MESH,
        ).wait_send()


class Leaps(Ring):
    def copy(self, rows, index, right, hop):
        step = 1 if right else -1
        kept = 0 if hop <= 2 else 2
        origin = lax.rem(self.me - step * kept + self.n, self.n)
        target = lax.rem(self.me + step * (hop - kept) + self.n, self.n)
        ref = self.buf.at[origin, rows]
        return pltpu.make_async_remote_copy(
            src_ref=ref,
            dst_ref=ref,
            send_sem=self.send_sem,
            recv_sem=self.recv_sem.at[index, 0 if right else 1, hop - 1],
            device_id={"tp": target},
            device_id_type=MESH,
        )

    def begin(self, rows, index):
        for hop in (2, 1):
            for right in (True, False):
                if hop <= self.hops(index, right):
                    self.copy(rows, index, right, hop).start()

    def pass_on(self, rows, index, hop):
        for right in (True, False):
            most = self.hops(index, right)
            if hop <= most:
                self.arrival(rows, index, right, hop)
                if hop == 2:
                    for later in range(most, 2, -1):
                        self.copy(rows, index, right, later).start()


def layer(
    nsp,
    ntp,
    cap,
    residual,
    queries,
    keys,
    values,
    segments,
    routes,
    route_weight,
    sinks,
    out_weight,
    gain,
    expert_gate,
    expert_up,
    expert_down,
    shared_gate,
    shared_up,
    shared_down,
    out,
    halo_k,
    halo_v,
    halo_m,
    proj_w,
    res,
    att,
    upd,
    normed,
    scatter,
    pick,
    outgoing,
    near_out,
    sums,
    rows_all,
    act_all,
    made,
    back,
    expert_in,
    expert_out,
    shared_in,
    shared_out,
    halo_send,
    halo_recv,
    w_send,
    w_recv,
    pair_send,
    pair_recv,
    att_send,
    att_recv,
    upd_send,
    upd_recv,
    sum_send,
    sum_recv,
    disp_send,
    near_send,
    disp_recv,
    rows_send,
    rows_recv,
    act_send,
    act_recv,
    ret_send,
    ret_recv,
    load_sem,
    chain_sem,
    all_in,
):
    me = lax.axis_index("sp")
    tp = lax.axis_index("tp")
    nz = nsp // CORES
    z, core = me // CORES, lax.rem(me, CORES)
    tokens = queries.shape[0]
    cols = res.shape[1]
    heads_wide = queries.shape[1]
    blocks = tokens // WINDOW
    slots = nsp * cap
    hidden = expert_gate.shape[2]
    sibling = z * CORES + lax.rem(core + 1, CORES)
    following = lax.rem(me + 1, nsp)

    col_start = pl.multiple_of(tp * cols, cols)
    loads = [
        (residual.at[:, pl.ds(col_start, cols)], res),
        (shared_gate, shared_in.at[:, pl.ds(0, hidden)]),
        (shared_up, shared_in.at[:, pl.ds(hidden, hidden)]),
        (expert_gate.at[0], expert_in.at[:, pl.ds(0, hidden)]),
        (expert_up.at[0], expert_in.at[:, pl.ds(hidden, hidden)]),
        (expert_down.at[0], expert_out),
        (shared_down, shared_out),
    ]
    loads = [pltpu.make_async_copy(src, dst, load_sem.at[i]) for i, (src, dst) in enumerate(loads)]
    for load in loads:
        load.start()

    def say(semaphore, where):
        pl.semaphore_signal(semaphore, inc=1, device_id=where, device_id_type=MESH)

    last = (me + 1) // nsp
    barrier = pltpu.get_barrier_semaphore()
    for d in range(1, ntp):
        say(barrier, {"tp": lax.rem(tp + d, ntp)})
    say(barrier, {"sp": sibling})

    @pl.when(core == 0)
    def _():
        say(barrier, {"sp": lax.rem(me + nsp - 1, nsp)})

    @pl.when(me == 1)
    def _():
        say(barrier, {"sp": nsp - 1})

    pl.semaphore_wait(barrier, ntp + core + last)

    @pl.when(me >= 3)
    def _():
        pl.semaphore_wait(chain_sem, 1)

    @pl.when((me >= 2) & (me < nsp - 1))
    def _():
        say(chain_sem, {"sp": following})

    @pl.when(me == nsp - 1)
    def _():
        reach = [min(j // CORES + 1, nz - 1 - j // CORES) for j in range(nsp - 1)]
        for j in sorted(range(nsp - 1), key=lambda j: -reach[j]):
            say(all_in, {"sp": j})

    tail = pl.ds(tokens - WINDOW, WINDOW)
    halo = [
        pltpu.make_async_remote_copy(
            src_ref=src,
            dst_ref=dst,
            send_sem=halo_send.at[i],
            recv_sem=halo_recv.at[i],
            device_id={"sp": following},
            device_id_type=MESH,
        )
        for i, (src, dst) in enumerate(
            [(keys.at[:, tail], halo_k), (values.at[:, tail], halo_v), (segments.at[:, tail], halo_m)]
        )
    ]

    @pl.when(me < nsp - 1)
    def _():
        for copy in halo:
            copy.start()


    part = heads_wide // CORES

    def weight_copy(d):
        target = lax.rem(tp + d, ntp)
        return pltpu.make_async_remote_copy(
            src_ref=out_weight.at[
                pl.ds(pl.multiple_of(core * part, part), part),
                pl.ds(pl.multiple_of(target * cols, cols), cols),
            ],
            dst_ref=proj_w.at[pl.ds(pl.multiple_of(tp * heads_wide + core * part, part), part)],
            send_sem=w_send.at[d - 1],
            recv_sem=w_recv.at[d - 1],
            device_id={"tp": target},
            device_id_type=MESH,
        )

    def weight_rows(d, which):
        source = lax.rem(tp - d + ntp, ntp)
        return proj_w.at[pl.ds(pl.multiple_of(source * heads_wide + which * part, part), part)]

    def pair_copy(d):
        ref = weight_rows(d, core)
        return pltpu.make_async_remote_copy(
            src_ref=ref,
            dst_ref=ref,
            send_sem=pair_send.at[d - 1],
            recv_sem=pair_recv.at[d - 1],
            device_id={"sp": sibling},
            device_id_type=MESH,
        )

    distances = sorted(range(1, ntp), key=lambda d: min(d, ntp - d))
    split = len(distances) // 2
    for d in distances[split:]:
        weight_copy(d).start()
    proj_w[pl.ds(pl.multiple_of(tp * heads_wide, heads_wide), heads_wide), :] = out_weight[
        :, pl.ds(col_start, cols)
    ]

    att_ring = Leaps(ntp, tp, att, att_send, att_recv)
    upd_ring = Ring(ntp, tp, upd, upd_send, upd_recv)
    seg_row = segments[...].astype(F32)
    weight_row = route_weight[...]
    col_meta = jnp.transpose(
        jnp.concatenate([seg_row, weight_row, jnp.zeros((5, tokens), F32)], axis=0)
    )
    q_pos = lax.broadcasted_iota(jnp.int32, (WINDOW, 2 * WINDOW), 0)
    k_pos = lax.broadcasted_iota(jnp.int32, (WINDOW, 2 * WINDOW), 1)
    offset = q_pos + WINDOW - k_pos
    band = (offset >= 0) & (offset < WINDOW)

    def attend(b, band_k, band_v, band_seg):
        rows = slice(b * WINDOW, (b + 1) * WINDOW)
        allowed = band & (col_meta[rows, 0:1] == band_seg)
        heads = []
        for h in range(heads_wide // HEAD_DIM):
            q = queries[rows, h * HEAD_DIM : (h + 1) * HEAD_DIM]
            scores = jnp.dot(q, band_k, preferred_element_type=F32) * HEAD_DIM ** (-0.5)
            masked = jnp.where(allowed, scores, -jnp.inf)
            sink = sinks[h]
            top = jnp.maximum(jnp.max(masked, axis=-1, keepdims=True), sink)
            terms = jnp.exp(masked - top)
            denominator = jnp.sum(terms, axis=-1, keepdims=True) + jnp.exp(sink - top)
            weights = (terms / denominator).astype(BF16)
            mixed = lax.dot_general(
                weights, band_v, (((1,), (1,)), ((), ())), preferred_element_type=F32
            )
            heads.append(mixed.astype(BF16))
        att[tp, rows, :] = jnp.concatenate(heads, axis=1)

    order = list(range(1, blocks)) + [0]
    span = [pl.ds(b * WINDOW, WINDOW) for b in range(blocks)]
    for b in order[:-1]:
        reach = slice((b - 1) * WINDOW, (b + 1) * WINDOW)
        attend(b, keys[:, reach], values[:, reach], seg_row[:, reach])
        att_ring.begin(span[b], b)
    for d in distances[:split]:
        weight_copy(d).start()

    @pl.when(me > 0)
    def _():
        for copy in halo:
            copy.wait_recv()

    @pl.when(me == 0)
    def _():
        for ref in (halo_k, halo_v, halo_m):
            ref[...] = jnp.zeros_like(ref)

    first = slice(0, WINDOW)
    halo_seg = jnp.where(me == 0, -1.0, halo_m[...].astype(F32))
    attend(
        0,
        jnp.concatenate([halo_k[...], keys[:, first]], axis=1),
        jnp.concatenate([halo_v[...], values[:, first]], axis=1),
        jnp.concatenate([halo_seg, seg_row[:, first]], axis=1),
    )
    att_ring.begin(span[0], 0)

    route_of = [routes[k : k + 1, :].astype(F32) for k in range(2)]
    experts = lax.broadcasted_iota(jnp.int32, (nsp, tokens), 0).astype(F32)
    named = [(experts == r).astype(F32) for r in route_of]
    earlier = lax.broadcasted_iota(jnp.int32, (tokens, tokens), 0)
    later = lax.broadcasted_iota(jnp.int32, (tokens, tokens), 1)
    before = (earlier < later).astype(F32).astype(BF16)
    counts = jnp.dot((named[0] + named[1]).astype(BF16), before, preferred_element_type=F32)
    slot_row = [
        r * cap + jnp.sum(counts * m, axis=0, keepdims=True) for r, m in zip(route_of, named)
    ]
    slot_down = lax.broadcasted_iota(jnp.int32, (slots, tokens), 0).astype(F32)
    hit = (slot_down == slot_row[0]) | (slot_down == slot_row[1])
    scatter[...] = jnp.where(hit, 1.0, 0.0).astype(BF16)
    slot_col = jnp.transpose(
        jnp.concatenate([slot_row[0], slot_row[1], jnp.zeros((6, tokens), F32)], axis=0)
    )
    slot_along = lax.broadcasted_iota(jnp.int32, (tokens, slots), 1).astype(F32)
    for k in range(2):
        pick[k, :, :] = jnp.where(slot_along == slot_col[:, k : k + 1], 1.0, 0.0).astype(BF16)

    def weight_arrival(d):
        weight_copy(d).wait_recv()
        pair_copy(d).start()

    hops = list(range(1, att_ring.longest() + 1))
    for hop in hops[1:2] + hops[:1] + hops[2:]:
        for b in order:
            att_ring.pass_on(span[b], b, hop)
        if hop == 1:
            for d in distances[split:] + distances[:split]:
                weight_arrival(d)
    for d in distances:
        pair_copy(d).wait_recv()
    loads[0].wait()

    for b in order:
        rows = slice(b * WINDOW, (b + 1) * WINDOW)
        total = jnp.zeros((WINDOW, cols), F32)
        for s in range(ntp):
            total += jnp.dot(
                att[s, rows, :],
                proj_w[s * heads_wide : (s + 1) * heads_wide, :],
                preferred_element_type=F32,
            )
        upd[tp, rows, :] = (res[rows, :].astype(F32) + total).astype(BF16)
    own_cols = upd[tp].astype(F32)
    squares = jnp.sum(own_cols * own_cols, axis=-1, keepdims=True)
    sums[tp] = jnp.transpose(jnp.broadcast_to(squares, (tokens, 128)))[0:8, :]

    def sum_copy(d):
        return pltpu.make_async_remote_copy(
            src_ref=sums.at[tp],
            dst_ref=sums.at[tp],
            send_sem=sum_send.at[d - 1],
            recv_sem=sum_recv.at[d - 1],
            device_id={"tp": lax.rem(tp + d, ntp)},
            device_id_type=MESH,
        )

    def sum_arrival(d):
        source = lax.rem(tp - d + ntp, ntp)
        pltpu.make_async_remote_copy(
            src_ref=sums.at[source],
            dst_ref=sums.at[source],
            send_sem=sum_send.at[d - 1],
            recv_sem=sum_recv.at[d - 1],
            device_id={"tp": source},
            device_id_type=MESH,
        ).wait_recv()

    for d in distances[::-1]:
        sum_copy(d).start()
    for b in order:
        upd_ring.begin(span[b], b)
    for d in range(1, ntp):
        sum_arrival(d)
    squares = sums[0]
    for s in range(1, ntp):
        squares += sums[s]
    inv_rms = jnp.transpose(lax.rsqrt(squares / (ntp * cols) + EPSILON))[:, 0:1]

    chips = send_order(nz)
    places = [(d, s) for d in chips for s in range(CORES) if (d, s) != (0, 0)]
    own_gain = gain[0:1, pl.ds(col_start, cols)]
    own_normed = (own_cols * inv_rms * own_gain).astype(BF16)
    outgoing[...] = jnp.dot(scatter[...], own_normed, preferred_element_type=F32).astype(BF16)

    def at_chip(d, s):
        return lax.rem(z + d + nz, nz) * CORES + lax.rem(core + s, CORES)

    def slot_block(index):
        return pl.ds(pl.multiple_of(index * cap, cap), cap)

    def dispatch_copy(i):
        d, s = places[i]
        target = at_chip(d, s)
        return pltpu.make_async_remote_copy(
            src_ref=outgoing.at[slot_block(target)],
            dst_ref=rows_all.at[tp, slot_block(me)],
            send_sem=disp_send,
            recv_sem=disp_recv.at[me],
            device_id={"sp": target},
            device_id_type=MESH,
        )

    chunk_sources = 2 * CORES
    chunks = nsp // chunk_sources
    own_chunk = me // chunk_sources

    @pl.when(me < nsp - 1)
    def _():
        pl.semaphore_wait(all_in, 1)

    for i in range(len(places)):
        far = at_chip(*places[i]) // chunk_sources != own_chunk

        @pl.when(far)
        def _():
            dispatch_copy(i).start()


    def block_wait(ref, sem):
        pltpu.make_async_remote_copy(
            src_ref=ref,
            dst_ref=ref,
            send_sem=disp_send,
            recv_sem=sem,
            device_id={"sp": me},
            device_id_type=MESH,
        ).wait_recv()

    act_ring = Ring(ntp, tp, act_all, act_send, act_recv)
    rows_ring = Ring(ntp, tp, rows_all, rows_send, rows_recv)

    def activate(gate_up):
        gate, up = gate_up[:, :hidden], gate_up[:, hidden:]
        return (gate / (1.0 + jnp.exp(-gate)) * up).astype(BF16)

    shared_chunk = chunks
    partners = [
        own_chunk * chunk_sources + lax.rem(me + k, chunk_sources) for k in range(1, chunk_sources)
    ]

    def near_copy(k):
        return pltpu.make_async_remote_copy(
            src_ref=near_out.at[:, pl.ds(k * cap, cap)],
            dst_ref=rows_all.at[:, slot_block(me)],
            send_sem=near_send,
            recv_sem=disp_recv.at[me],
            device_id={"sp": partners[k]},
            device_id_type=MESH,
        )

    def near_rows():
        chosen = jnp.concatenate(
            [scatter[slot_block(target), :] for target in partners + [me]], axis=0
        )
        sent = len(partners) * cap
        for s in range(ntp):
            normed[s] = (
                upd[s].astype(F32) * inv_rms * gain[0:1, s * cols : (s + 1) * cols]
            ).astype(BF16)
            picked = jnp.dot(chosen, normed[s], preferred_element_type=F32).astype(BF16)
            near_out[s, :, :] = picked[:sent]
            rows_all[s, slot_block(me), :] = picked[sent:]
        for k in range(len(partners)):
            near_copy(k).start()

    def places_of(q):
        return range(q * chunk_sources, (q + 1) * chunk_sources)

    def rows_of(q):
        if q == shared_chunk:
            return slots, tokens
        return q * chunk_sources * cap, chunk_sources * cap

    def span_of(q):
        return pl.ds(*rows_of(q))

    def upd_hop(hop):
        for b in order:
            upd_ring.pass_on(span[b], b, hop)

    def shared_units():
        total = jnp.zeros((tokens, 2 * hidden), F32)
        for s in range(ntp):
            total += jnp.dot(
                normed[s], shared_in[s * cols : (s + 1) * cols, :], preferred_element_type=F32
            )
        act_all[tp, slots : slots + tokens, :] = activate(total)
        act_ring.begin(span_of(shared_chunk), shared_chunk)

    for load in loads[1:]:
        load.wait()

    def ready(q):
        @pl.when(own_chunk != q)
        def _():
            for source in places_of(q):
                block_wait(rows_all.at[tp, pl.ds(source * cap, cap)], disp_recv.at[source])
            rows_ring.begin(span_of(q), q)

    def rows_hop(q, hop):
        @pl.when(own_chunk != q)
        def _():
            rows_ring.pass_on(span_of(q), q, hop)

    def hidden_units(q):
        @pl.when(own_chunk == q)
        def _():
            for source in partners:
                block_wait(rows_all.at[:, slot_block(source)], disp_recv.at[source])

        start, count = rows_of(q)
        total = jnp.zeros((count, 2 * hidden), F32)
        for s in range(ntp):
            total += jnp.dot(
                rows_all[s, start : start + count, :],
                expert_in[s * cols : (s + 1) * cols, :],
                preferred_element_type=F32,
            )
        act_all[tp, start : start + count, :] = activate(total)
        act_ring.begin(span_of(q), q)

    def act_hop(q, hop):
        act_ring.pass_on(span_of(q), q, hop)

    def return_copy(source):
        return pltpu.make_async_remote_copy(
            src_ref=made.at[pl.ds(source * cap, cap)],
            dst_ref=back.at[slot_block(me)],
            send_sem=ret_send,
            recv_sem=ret_recv.at[me],
            device_id={"sp": source},
            device_id_type=MESH,
        )

    def outputs(q):
        start, count = rows_of(q)
        total = jnp.zeros((count, cols), F32)
        for s in range(ntp):
            total += jnp.dot(
                act_all[s, start : start + count, :],
                expert_out[s * hidden : (s + 1) * hidden, :],
                preferred_element_type=F32,
            )
        made[start : start + count, :] = total.astype(BF16)
        for source in places_of(q):

            @pl.when(me == source)
            def _():
                back[slot_block(me), :] = made[source * cap : (source + 1) * cap, :]

            @pl.when(me != source)
            def _():
                return_copy(source).start()

    row_hop, act_hop_time, upd_hop_time, period = 5.0, 5.0, 3.0, 7.4
    longest = rows_ring.longest()
    steps = []
    for hop in range(1, longest + 1):
        steps.append((hop * upd_hop_time, functools.partial(upd_hop, hop)))

    steps.append((longest * upd_hop_time + 0.1, functools.partial(near_rows)))

    def act_steps(at, q):
        for hop in range(1, longest + 1):
            steps.append((at + hop * act_hop_time, functools.partial(act_hop, q, hop)))
        at += longest * act_hop_time + 0.1
        if q != shared_chunk:
            steps.append((at, functools.partial(outputs, q)))

    in_turn = list(range(1, min(3, chunks))) + [0] + list(range(3, chunks))
    at = 8.0
    for q in in_turn:
        steps.append((at, functools.partial(ready, q)))
        for hop in range(1, longest + 1):
            steps.append((at + hop * row_hop, functools.partial(rows_hop, q, hop)))
        done = at + longest * row_hop + 0.1
        steps.append((done, functools.partial(hidden_units, q)))
        act_steps(done, q)
        at += period
    at = max(at, longest * upd_hop_time) + 13.0
    steps.append((at, functools.partial(shared_units)))
    act_steps(at, shared_chunk)
    for _, step in sorted(steps, key=lambda step: step[0]):
        step()

    total = upd[tp].astype(F32)
    for s in range(ntp):
        total += jnp.dot(
            act_all[s, slots : slots + tokens, :],
            shared_out[s * hidden : (s + 1) * hidden, :],
            preferred_element_type=F32,
        )
    for expert in range(nsp):

        @pl.when(me != expert)
        def _():
            block_wait(back.at[pl.ds(expert * cap, cap)], ret_recv.at[expert])

    for k in range(2):
        picked = jnp.dot(pick[k], back[...], preferred_element_type=F32)
        total += picked * col_meta[:, 1 + k : 2 + k]
    out[...] = total.astype(BF16)

    @pl.when(me < nsp - 1)
    def _():
        for copy in halo:
            copy.wait_send()

    for d in distances:
        weight_copy(d).wait_send()
        pair_copy(d).wait_send()
    for d in range(1, ntp):
        sum_copy(d).wait_send()
    att_ring.finish(tokens)
    upd_ring.finish(tokens)
    rows_ring.finish((nsp - chunk_sources) * cap)
    act_ring.finish(slots + tokens)
    sent = [
        (outgoing.at[pl.ds(0, (nsp - chunk_sources) * cap)], disp_send),
        (near_out, near_send),
        (made.at[pl.ds(0, (nsp - 1) * cap)], ret_send),
    ]
    for ref, sem in sent:
        pltpu.make_async_remote_copy(
            src_ref=ref,
            dst_ref=ref,
            send_sem=sem,
            recv_sem=ret_recv.at[0],
            device_id={"sp": me},
            device_id_type=MESH,
        ).wait_send()


def shards(
    nsp,
    ntp,
    residual,
    queries,
    keys,
    values,
    segments,
    routes,
    route_weight,
    sinks,
    out_weight,
    norm_gain,
    expert_gate,
    expert_up,
    expert_down,
    shared_gate,
    shared_up,
    shared_down,
):
    tokens, width = residual.shape
    cols = width // ntp
    hidden = expert_gate.shape[2]
    heads_wide = queries.shape[1]
    cap = 2 * tokens * routes.shape[1] // nsp
    slots = nsp * cap
    longest = ntp // 2
    chunks = nsp // (2 * CORES)
    vmem = pl.BlockSpec(memory_space=pltpu.VMEM)
    smem = pl.BlockSpec(memory_space=pltpu.SMEM)
    anywhere = pl.BlockSpec(memory_space=pl.ANY)
    dma = pltpu.SemaphoreType.DMA
    return pl.pallas_call(
        functools.partial(layer, nsp, ntp, cap),
        out_shape=jax.ShapeDtypeStruct((tokens, cols), BF16),
        in_specs=[anywhere] + [vmem] * 6 + [smem, vmem, vmem] + [anywhere] * 6,
        out_specs=vmem,
        scratch_shapes=[
            pltpu.VMEM((keys.shape[1], WINDOW), BF16),
            pltpu.VMEM((values.shape[1], WINDOW), BF16),
            pltpu.VMEM((1, WINDOW), jnp.int32),
            pltpu.VMEM((ntp * heads_wide, cols), BF16),
            pltpu.VMEM((tokens, cols), BF16),
            pltpu.VMEM((ntp, tokens, heads_wide), BF16),
            pltpu.VMEM((ntp, tokens, cols), BF16),
            pltpu.VMEM((ntp, tokens, cols), BF16),
            pltpu.VMEM((slots, tokens), BF16),
            pltpu.VMEM((2, tokens, slots), BF16),
            pltpu.VMEM((slots, cols), BF16),
            pltpu.VMEM((ntp, (2 * CORES - 1) * cap, cols), BF16),
            pltpu.VMEM((ntp, 8, tokens), F32),
            pltpu.VMEM((ntp, slots, cols), BF16),
            pltpu.VMEM((ntp, slots + tokens, hidden), BF16),
            pltpu.VMEM((slots, cols), BF16),
            pltpu.VMEM((slots, cols), BF16),
            pltpu.VMEM((width, 2 * hidden), BF16),
            pltpu.VMEM((ntp * hidden, cols), BF16),
            pltpu.VMEM((width, 2 * hidden), BF16),
            pltpu.VMEM((ntp * hidden, cols), BF16),
            dma((3,)),
            dma((3,)),
            dma((ntp - 1,)),
            dma((ntp - 1,)),
            dma((ntp - 1,)),
            dma((ntp - 1,)),
            dma,
            dma((tokens // WINDOW, 2, longest)),
            dma,
            dma((tokens // WINDOW, 2, longest)),
            dma((ntp - 1,)),
            dma((ntp - 1,)),
            dma,
            dma,
            dma((nsp,)),
            dma,
            dma((chunks, 2, longest)),
            dma,
            dma((chunks + 1, 2, longest)),
            dma,
            dma((nsp,)),
            dma((7,)),
            pltpu.SemaphoreType.REGULAR,
            pltpu.SemaphoreType.REGULAR,
        ],
        compiler_params=pltpu.CompilerParams(collective_id=0, has_side_effects=True),
        name="layer",
    )(
        residual,
        queries,
        keys.T,
        values.T,
        segments.reshape(1, tokens),
        routes.T,
        route_weight.T,
        sinks,
        out_weight,
        norm_gain.reshape(1, width),
        expert_gate,
        expert_up,
        expert_down,
        shared_gate,
        shared_up,
        shared_down,
    )


def solution(mesh):
    in_specs = (
        P(GRP_SP, None),
        P(GRP_SP, "tp"),
        P(GRP_SP, "tp"),
        P(GRP_SP, "tp"),
        P(GRP_SP),
        P(GRP_SP, None),
        P(GRP_SP, None),
        P("tp"),
        P("tp", None),
        P(),
        P("sp", None, "tp"),
        P("sp", None, "tp"),
        P("sp", None, "tp"),
        P(None, "tp"),
        P(None, "tp"),
        P(None, "tp"),
    )
    return jax.shard_map(
        functools.partial(shards, mesh.shape["sp"], mesh.shape["tp"]),
        mesh=mesh,
        in_specs=in_specs,
        out_specs=P(GRP_SP, "tp"),
        check_vma=False,
    )
```

```python
import functools

import jax
import jax.numpy as jnp
from jax import lax
from jax.experimental import pallas as pl
from jax.experimental.pallas import tpu as pltpu
from jax.sharding import PartitionSpec as P

HEAD_DIM = 64
WINDOW = 128
CORES = 2
GRP_SP = ("grp", "sp")
EPSILON = 1e-06
MESH = pl.DeviceIdType.MESH
BF16 = jnp.bfloat16
F32 = jnp.float32


def send_order(nz):
    spread = [d if d <= nz // 2 else d - nz for d in range(nz)]
    by_reach = sorted(spread, key=lambda d: (abs(d), -d))
    order = []
    while by_reach:
        order.append(by_reach.pop(0))
        if by_reach:
            order.append(by_reach.pop(0))
        if by_reach:
            order.append(by_reach.pop())
    return order


class Ring:
    def __init__(self, n, me, buf, send_sem, recv_sem):
        self.n, self.me, self.buf, self.send_sem, self.recv_sem = n, me, buf, send_sem, recv_sem

    def hops(self, turn, right):
        longer = self.n // 2
        return longer if right == (turn % 2 == 0) else self.n - 1 - longer

    def copy(self, rows, index, right, hop):
        step = 1 if right else -1
        origin = lax.rem(self.me - step * (hop - 1) + self.n, self.n)
        target = lax.rem(self.me + step + self.n, self.n)
        ref = self.buf.at[origin, rows]
        return pltpu.make_async_remote_copy(
            src_ref=ref,
            dst_ref=ref,
            send_sem=self.send_sem,
            recv_sem=self.recv_sem.at[index, 0 if right else 1, hop - 1],
            device_id={"tp": target},
            device_id_type=MESH,
        )

    def arrival(self, rows, index, right, hop):
        step = 1 if right else -1
        origin = lax.rem(self.me - step * hop + self.n, self.n)
        ref = self.buf.at[origin, rows]
        pltpu.make_async_remote_copy(
            src_ref=ref,
            dst_ref=ref,
            send_sem=self.send_sem,
            recv_sem=self.recv_sem.at[index, 0 if right else 1, hop - 1],
            device_id={"tp": self.me},
            device_id_type=MESH,
        ).wait_recv()

    def begin(self, rows, index):
        for right in (True, False):
            if self.hops(index, right) > 0:
                self.copy(rows, index, right, 1).start()

    def pass_on(self, rows, index, hop):
        for right in (True, False):
            most = self.hops(index, right)
            if hop <= most:
                self.arrival(rows, index, right, hop)
                if hop < most:
                    self.copy(rows, index, right, hop + 1).start()

    def longest(self):
        return self.n // 2

    def finish(self, rows):
        ref = self.buf.at[pl.ds(0, self.n - 1), pl.ds(0, rows)]
        pltpu.make_async_remote_copy(
            src_ref=ref,
            dst_ref=ref,
            send_sem=self.send_sem,
            recv_sem=self.recv_sem.at[0, 0, 0],
            device_id={"tp": self.me},
            device_id_type=MESH,
        ).wait_send()


class Leaps(Ring):
    def copy(self, rows, index, right, hop):
        step = 1 if right else -1
        kept = 0 if hop <= 2 else 2
        origin = lax.rem(self.me - step * kept + self.n, self.n)
        target = lax.rem(self.me + step * (hop - kept) + self.n, self.n)
        ref = self.buf.at[origin, rows]
        return pltpu.make_async_remote_copy(
            src_ref=ref,
            dst_ref=ref,
            send_sem=self.send_sem,
            recv_sem=self.recv_sem.at[index, 0 if right else 1, hop - 1],
            device_id={"tp": target},
            device_id_type=MESH,
        )

    def begin(self, rows, index):
        for hop in (2, 1):
            for right in (True, False):
                if hop <= self.hops(index, right):
                    self.copy(rows, index, right, hop).start()

    def pass_on(self, rows, index, hop):
        for right in (True, False):
            most = self.hops(index, right)
            if hop <= most:
                self.arrival(rows, index, right, hop)
                if hop == 2:
                    for later in range(most, 2, -1):
                        self.copy(rows, index, right, later).start()


def layer(
    nsp,
    ntp,
    cap,
    residual,
    queries,
    keys,
    values,
    segments,
    routes,
    route_weight,
    sinks,
    out_weight,
    gain,
    expert_gate,
    expert_up,
    expert_down,
    shared_gate,
    shared_up,
    shared_down,
    out,
    halo_k,
    halo_v,
    halo_m,
    proj_w,
    res,
    att,
    upd,
    normed,
    scatter,
    pick,
    outgoing,
    near_out,
    sums,
    rows_all,
    act_all,
    made,
    back,
    expert_in,
    expert_out,
    shared_in,
    shared_out,
    halo_send,
    halo_recv,
    w_send,
    w_recv,
    pair_send,
    pair_recv,
    att_send,
    att_recv,
    upd_send,
    upd_recv,
    sum_send,
    sum_recv,
    disp_send,
    near_send,
    disp_recv,
    rows_send,
    rows_recv,
    act_send,
    act_recv,
    ret_send,
    ret_recv,
    load_sem,
    chain_sem,
    all_in,
):
    me = lax.axis_index("sp")
    tp = lax.axis_index("tp")
    nz = nsp // CORES
    z, core = me // CORES, lax.rem(me, CORES)
    tokens = queries.shape[0]
    cols = res.shape[1]
    heads_wide = queries.shape[1]
    blocks = tokens // WINDOW
    slots = nsp * cap
    hidden = expert_gate.shape[2]
    sibling = z * CORES + lax.rem(core + 1, CORES)
    following = lax.rem(me + 1, nsp)

    col_start = pl.multiple_of(tp * cols, cols)
    loads = [
        (residual.at[:, pl.ds(col_start, cols)], res),
        (shared_gate, shared_in.at[:, pl.ds(0, hidden)]),
        (shared_up, shared_in.at[:, pl.ds(hidden, hidden)]),
        (expert_gate.at[0], expert_in.at[:, pl.ds(0, hidden)]),
        (expert_up.at[0], expert_in.at[:, pl.ds(hidden, hidden)]),
        (expert_down.at[0], expert_out),
        (shared_down, shared_out),
    ]
    loads = [pltpu.make_async_copy(src, dst, load_sem.at[i]) for i, (src, dst) in enumerate(loads)]
    for load in loads:
        load.start()

    def say(semaphore, where):
        pl.semaphore_signal(semaphore, inc=1, device_id=where, device_id_type=MESH)

    last = (me + 1) // nsp
    barrier = pltpu.get_barrier_semaphore()
    for d in range(1, ntp):
        say(barrier, {"tp": lax.rem(tp + d, ntp)})
    say(barrier, {"sp": sibling})

    @pl.when(core == 0)
    def _():
        say(barrier, {"sp": lax.rem(me + nsp - 1, nsp)})

    @pl.when(me == 1)
    def _():
        say(barrier, {"sp": nsp - 1})

    pl.semaphore_wait(barrier, ntp + core + last)

    @pl.when(me >= 3)
    def _():
        pl.semaphore_wait(chain_sem, 1)

    @pl.when((me >= 2) & (me < nsp - 1))
    def _():
        say(chain_sem, {"sp": following})

    @pl.when(me == nsp - 1)
    def _():
        reach = [min(j // CORES + 1, nz - 1 - j // CORES) for j in range(nsp - 1)]
        for j in sorted(range(nsp - 1), key=lambda j: -reach[j]):
            say(all_in, {"sp": j})

    tail = pl.ds(tokens - WINDOW, WINDOW)
    halo = [
        pltpu.make_async_remote_copy(
            src_ref=src,
            dst_ref=dst,
            send_sem=halo_send.at[i],
            recv_sem=halo_recv.at[i],
            device_id={"sp": following},
            device_id_type=MESH,
        )
        for i, (src, dst) in enumerate(
            [(keys.at[:, tail], halo_k), (values.at[:, tail], halo_v), (segments.at[:, tail], halo_m)]
        )
    ]

    @pl.when(me < nsp - 1)
    def _():
        for copy in halo:
            copy.start()


    part = heads_wide // CORES

    def weight_copy(d):
        target = lax.rem(tp + d, ntp)
        return pltpu.make_async_remote_copy(
            src_ref=out_weight.at[
                pl.ds(pl.multiple_of(core * part, part), part),
                pl.ds(pl.multiple_of(target * cols, cols), cols),
            ],
            dst_ref=proj_w.at[pl.ds(pl.multiple_of(tp * heads_wide + core * part, part), part)],
            send_sem=w_send.at[d - 1],
            recv_sem=w_recv.at[d - 1],
            device_id={"tp": target},
            device_id_type=MESH,
        )

    def weight_rows(d, which):
        source = lax.rem(tp - d + ntp, ntp)
        return proj_w.at[pl.ds(pl.multiple_of(source * heads_wide + which * part, part), part)]

    def pair_copy(d):
        ref = weight_rows(d, core)
        return pltpu.make_async_remote_copy(
            src_ref=ref,
            dst_ref=ref,
            send_sem=pair_send.at[d - 1],
            recv_sem=pair_recv.at[d - 1],
            device_id={"sp": sibling},
            device_id_type=MESH,
        )

    distances = sorted(range(1, ntp), key=lambda d: min(d, ntp - d))
    split = len(distances) // 2
    for d in distances[split:]:
        weight_copy(d).start()
    proj_w[pl.ds(pl.multiple_of(tp * heads_wide, heads_wide), heads_wide), :] = out_weight[
        :, pl.ds(col_start, cols)
    ]

    att_ring = Leaps(ntp, tp, att, att_send, att_recv)
    upd_ring = Ring(ntp, tp, upd, upd_send, upd_recv)
    seg_row = segments[...].astype(F32)
    weight_row = route_weight[...]
    col_meta = jnp.transpose(
        jnp.concatenate([seg_row, weight_row, jnp.zeros((5, tokens), F32)], axis=0)
    )
    q_pos = lax.broadcasted_iota(jnp.int32, (WINDOW, 2 * WINDOW), 0)
    k_pos = lax.broadcasted_iota(jnp.int32, (WINDOW, 2 * WINDOW), 1)
    offset = q_pos + WINDOW - k_pos
    band = (offset >= 0) & (offset < WINDOW)

    def attend(b, band_k, band_v, band_seg):
        rows = slice(b * WINDOW, (b + 1) * WINDOW)
        allowed = band & (col_meta[rows, 0:1] == band_seg)
        heads = []
        for h in range(heads_wide // HEAD_DIM):
            q = queries[rows, h * HEAD_DIM : (h + 1) * HEAD_DIM]
            scores = jnp.dot(q, band_k, preferred_element_type=F32) * HEAD_DIM ** (-0.5)
            masked = jnp.where(allowed, scores, -jnp.inf)
            sink = sinks[h]
            top = jnp.maximum(jnp.max(masked, axis=-1, keepdims=True), sink)
            terms = jnp.exp(masked - top)
            denominator = jnp.sum(terms, axis=-1, keepdims=True) + jnp.exp(sink - top)
            weights = (terms / denominator).astype(BF16)
            mixed = lax.dot_general(
                weights, band_v, (((1,), (1,)), ((), ())), preferred_element_type=F32
            )
            heads.append(mixed.astype(BF16))
        att[tp, rows, :] = jnp.concatenate(heads, axis=1)

    order = list(range(1, blocks)) + [0]
    span = [pl.ds(b * WINDOW, WINDOW) for b in range(blocks)]
    for b in order[:-1]:
        reach = slice((b - 1) * WINDOW, (b + 1) * WINDOW)
        attend(b, keys[:, reach], values[:, reach], seg_row[:, reach])
        att_ring.begin(span[b], b)
    for d in distances[:split]:
        weight_copy(d).start()

    @pl.when(me > 0)
    def _():
        for copy in halo:
            copy.wait_recv()

    @pl.when(me == 0)
    def _():
        for ref in (halo_k, halo_v, halo_m):
            ref[...] = jnp.zeros_like(ref)

    first = slice(0, WINDOW)
    halo_seg = jnp.where(me == 0, -1.0, halo_m[...].astype(F32))
    attend(
        0,
        jnp.concatenate([halo_k[...], keys[:, first]], axis=1),
        jnp.concatenate([halo_v[...], values[:, first]], axis=1),
        jnp.concatenate([halo_seg, seg_row[:, first]], axis=1),
    )
    att_ring.begin(span[0], 0)

    route_of = [routes[k : k + 1, :].astype(F32) for k in range(2)]
    experts = lax.broadcasted_iota(jnp.int32, (nsp, tokens), 0).astype(F32)
    named = [(experts == r).astype(F32) for r in route_of]
    earlier = lax.broadcasted_iota(jnp.int32, (tokens, tokens), 0)
    later = lax.broadcasted_iota(jnp.int32, (tokens, tokens), 1)
    before = (earlier < later).astype(F32).astype(BF16)
    counts = jnp.dot((named[0] + named[1]).astype(BF16), before, preferred_element_type=F32)
    slot_row = [
        r * cap + jnp.sum(counts * m, axis=0, keepdims=True) for r, m in zip(route_of, named)
    ]
    slot_down = lax.broadcasted_iota(jnp.int32, (slots, tokens), 0).astype(F32)
    hit = (slot_down == slot_row[0]) | (slot_down == slot_row[1])
    scatter[...] = jnp.where(hit, 1.0, 0.0).astype(BF16)
    slot_col = jnp.transpose(
        jnp.concatenate([slot_row[0], slot_row[1], jnp.zeros((6, tokens), F32)], axis=0)
    )
    slot_along = lax.broadcasted_iota(jnp.int32, (tokens, slots), 1).astype(F32)
    for k in range(2):
        pick[k, :, :] = jnp.where(slot_along == slot_col[:, k : k + 1], 1.0, 0.0).astype(BF16)

    def weight_arrival(d):
        weight_copy(d).wait_recv()
        pair_copy(d).start()

    hops = list(range(1, att_ring.longest() + 1))
    for hop in hops[1:2] + hops[:1] + hops[2:]:
        for b in order:
            att_ring.pass_on(span[b], b, hop)
        if hop == 1:
            for d in distances[split:] + distances[:split]:
                weight_arrival(d)
    for d in distances:
        pair_copy(d).wait_recv()
    loads[0].wait()

    for b in order:
        rows = slice(b * WINDOW, (b + 1) * WINDOW)
        total = jnp.zeros((WINDOW, cols), F32)
        for s in range(ntp):
            total += jnp.dot(
                att[s, rows, :],
                proj_w[s * heads_wide : (s + 1) * heads_wide, :],
                preferred_element_type=F32,
            )
        upd[tp, rows, :] = (res[rows, :].astype(F32) + total).astype(BF16)
    own_cols = upd[tp].astype(F32)
    squares = jnp.sum(own_cols * own_cols, axis=-1, keepdims=True)
    sums[tp] = jnp.transpose(jnp.broadcast_to(squares, (tokens, 128)))[0:8, :]

    def sum_copy(d):
        return pltpu.make_async_remote_copy(
            src_ref=sums.at[tp],
            dst_ref=sums.at[tp],
            send_sem=sum_send.at[d - 1],
            recv_sem=sum_recv.at[d - 1],
            device_id={"tp": lax.rem(tp + d, ntp)},
            device_id_type=MESH,
        )

    def sum_arrival(d):
        source = lax.rem(tp - d + ntp, ntp)
        pltpu.make_async_remote_copy(
            src_ref=sums.at[source],
            dst_ref=sums.at[source],
            send_sem=sum_send.at[d - 1],
            recv_sem=sum_recv.at[d - 1],
            device_id={"tp": source},
            device_id_type=MESH,
        ).wait_recv()

    for d in distances[::-1]:
        sum_copy(d).start()
    for b in order:
        upd_ring.begin(span[b], b)
    for d in range(1, ntp):
        sum_arrival(d)
    squares = sums[0]
    for s in range(1, ntp):
        squares += sums[s]
    inv_rms = jnp.transpose(lax.rsqrt(squares / (ntp * cols) + EPSILON))[:, 0:1]

    chips = send_order(nz)
    places = [(d, s) for d in chips for s in range(CORES) if (d, s) != (0, 0)]
    own_gain = gain[0:1, pl.ds(col_start, cols)]
    own_normed = (own_cols * inv_rms * own_gain).astype(BF16)
    outgoing[...] = jnp.dot(scatter[...], own_normed, preferred_element_type=F32).astype(BF16)

    def at_chip(d, s):
        return lax.rem(z + d + nz, nz) * CORES + lax.rem(core + s, CORES)

    def slot_block(index):
        return pl.ds(pl.multiple_of(index * cap, cap), cap)

    def dispatch_copy(i):
        d, s = places[i]
        target = at_chip(d, s)
        return pltpu.make_async_remote_copy(
            src_ref=outgoing.at[slot_block(target)],
            dst_ref=rows_all.at[tp, slot_block(me)],
            send_sem=disp_send,
            recv_sem=disp_recv.at[me],
            device_id={"sp": target},
            device_id_type=MESH,
        )

    chunk_sources = 2 * CORES
    chunks = nsp // chunk_sources
    own_chunk = me // chunk_sources

    @pl.when(me < nsp - 1)
    def _():
        pl.semaphore_wait(all_in, 1)

    for i in range(len(places)):
        far = at_chip(*places[i]) // chunk_sources != own_chunk

        @pl.when(far)
        def _():
            dispatch_copy(i).start()


    def block_wait(ref, sem):
        pltpu.make_async_remote_copy(
            src_ref=ref,
            dst_ref=ref,
            send_sem=disp_send,
            recv_sem=sem,
            device_id={"sp": me},
            device_id_type=MESH,
        ).wait_recv()

    act_ring = Ring(ntp, tp, act_all, act_send, act_recv)
    rows_ring = Ring(ntp, tp, rows_all, rows_send, rows_recv)

    def activate(gate_up):
        gate, up = gate_up[:, :hidden], gate_up[:, hidden:]
        return (gate / (1.0 + jnp.exp(-gate)) * up).astype(BF16)

    shared_chunk = chunks
    partners = [
        own_chunk * chunk_sources + lax.rem(me + k, chunk_sources) for k in range(1, chunk_sources)
    ]

    def near_copy(k):
        return pltpu.make_async_remote_copy(
            src_ref=near_out.at[:, pl.ds(k * cap, cap)],
            dst_ref=rows_all.at[:, slot_block(me)],
            send_sem=near_send,
            recv_sem=disp_recv.at[me],
            device_id={"sp": partners[k]},
            device_id_type=MESH,
        )

    def near_rows():
        chosen = jnp.concatenate(
            [scatter[slot_block(target), :] for target in partners + [me]], axis=0
        )
        sent = len(partners) * cap
        for s in range(ntp):
            normed[s] = (
                upd[s].astype(F32) * inv_rms * gain[0:1, s * cols : (s + 1) * cols]
            ).astype(BF16)
            picked = jnp.dot(chosen, normed[s], preferred_element_type=F32).astype(BF16)
            near_out[s, :, :] = picked[:sent]
            rows_all[s, slot_block(me), :] = picked[sent:]
        for k in range(len(partners)):
            near_copy(k).start()

    half = me // (nsp // 2)

    def taken(q):
        if q == chunks - 2:
            return q + half
        return q - half if q == chunks - 1 else q

    def places_of(q):
        return [taken(q) * chunk_sources + k for k in range(chunk_sources)]

    def rows_of(q):
        if q == shared_chunk:
            return slots, tokens
        return pl.multiple_of(taken(q) * chunk_sources * cap, cap), chunk_sources * cap

    def span_of(q):
        return pl.ds(*rows_of(q))

    def upd_hop(hop):
        for b in order:
            upd_ring.pass_on(span[b], b, hop)

    def shared_units():
        total = jnp.zeros((tokens, 2 * hidden), F32)
        for s in range(ntp):
            total += jnp.dot(
                normed[s], shared_in[s * cols : (s + 1) * cols, :], preferred_element_type=F32
            )
        act_all[tp, slots : slots + tokens, :] = activate(total)
        act_ring.begin(span_of(shared_chunk), shared_chunk)

    for load in loads[1:]:
        load.wait()

    def ready(q):
        @pl.when(own_chunk != taken(q))
        def _():
            for source in places_of(q):
                block_wait(rows_all.at[tp, slot_block(source)], disp_recv.at[source])
            rows_ring.begin(span_of(q), q)

    def rows_hop(q, hop):
        @pl.when(own_chunk != taken(q))
        def _():
            rows_ring.pass_on(span_of(q), q, hop)

    def hidden_units(q):
        @pl.when(own_chunk == taken(q))
        def _():
            for source in partners:
                block_wait(rows_all.at[:, slot_block(source)], disp_recv.at[source])

        start, count = rows_of(q)
        total = jnp.zeros((count, 2 * hidden), F32)
        for s in range(ntp):
            total += jnp.dot(
                rows_all[s, pl.ds(start, count), :],
                expert_in[s * cols : (s + 1) * cols, :],
                preferred_element_type=F32,
            )
        act_all[tp, pl.ds(start, count), :] = activate(total)
        act_ring.begin(span_of(q), q)

    def act_hop(q, hop):
        act_ring.pass_on(span_of(q), q, hop)

    def return_copy(source):
        return pltpu.make_async_remote_copy(
            src_ref=made.at[slot_block(source)],
            dst_ref=back.at[slot_block(me)],
            send_sem=ret_send,
            recv_sem=ret_recv.at[me],
            device_id={"sp": source},
            device_id_type=MESH,
        )

    def outputs(q):
        start, count = rows_of(q)
        total = jnp.zeros((count, cols), F32)
        for s in range(ntp):
            total += jnp.dot(
                act_all[s, pl.ds(start, count), :],
                expert_out[s * hidden : (s + 1) * hidden, :],
                preferred_element_type=F32,
            )
        made[pl.ds(start, count), :] = total.astype(BF16)
        for source in places_of(q):

            @pl.when(me == source)
            def _():
                back[slot_block(me), :] = made[slot_block(source), :]

            @pl.when(me != source)
            def _():
                return_copy(source).start()

    row_hop, act_hop_time, upd_hop_time, period = 5.0, 5.0, 3.0, 7.4
    longest = rows_ring.longest()
    steps = []
    for hop in range(1, longest + 1):
        steps.append((hop * upd_hop_time, functools.partial(upd_hop, hop)))

    steps.append((longest * upd_hop_time + 0.1, functools.partial(near_rows)))

    def act_steps(at, q):
        for hop in range(1, longest + 1):
            steps.append((at + hop * act_hop_time, functools.partial(act_hop, q, hop)))
        at += longest * act_hop_time + 0.1
        if q != shared_chunk:
            steps.append((at, functools.partial(outputs, q)))

    in_turn = list(range(1, min(3, chunks))) + [0] + list(range(3, chunks))
    at = 9.5
    for q in in_turn:
        steps.append((at, functools.partial(ready, q)))
        for hop in range(1, longest + 1):
            steps.append((at + hop * row_hop, functools.partial(rows_hop, q, hop)))
        done = at + longest * row_hop + 0.1
        steps.append((done, functools.partial(hidden_units, q)))
        act_steps(done, q)
        at += period
    at = max(at, longest * upd_hop_time) + 13.0
    steps.append((at, functools.partial(shared_units)))
    act_steps(at, shared_chunk)
    for _, step in sorted(steps, key=lambda step: step[0]):
        step()

    total = upd[tp].astype(F32)
    for s in range(ntp):
        total += jnp.dot(
            act_all[s, slots : slots + tokens, :],
            shared_out[s * hidden : (s + 1) * hidden, :],
            preferred_element_type=F32,
        )
    for expert in range(nsp):

        @pl.when(me != expert)
        def _():
            block_wait(back.at[pl.ds(expert * cap, cap)], ret_recv.at[expert])

    for k in range(2):
        picked = jnp.dot(pick[k], back[...], preferred_element_type=F32)
        total += picked * col_meta[:, 1 + k : 2 + k]
    out[...] = total.astype(BF16)

    @pl.when(me < nsp - 1)
    def _():
        for copy in halo:
            copy.wait_send()

    for d in distances:
        weight_copy(d).wait_send()
        pair_copy(d).wait_send()
    for d in range(1, ntp):
        sum_copy(d).wait_send()
    att_ring.finish(tokens)
    upd_ring.finish(tokens)
    rows_ring.finish((nsp - chunk_sources) * cap)
    act_ring.finish(slots + tokens)
    sent = [
        (outgoing.at[pl.ds(0, (nsp - chunk_sources) * cap)], disp_send),
        (near_out, near_send),
        (made.at[pl.ds(0, (nsp - 1) * cap)], ret_send),
    ]
    for ref, sem in sent:
        pltpu.make_async_remote_copy(
            src_ref=ref,
            dst_ref=ref,
            send_sem=sem,
            recv_sem=ret_recv.at[0],
            device_id={"sp": me},
            device_id_type=MESH,
        ).wait_send()


def shards(
    nsp,
    ntp,
    residual,
    queries,
    keys,
    values,
    segments,
    routes,
    route_weight,
    sinks,
    out_weight,
    norm_gain,
    expert_gate,
    expert_up,
    expert_down,
    shared_gate,
    shared_up,
    shared_down,
):
    tokens, width = residual.shape
    cols = width // ntp
    hidden = expert_gate.shape[2]
    heads_wide = queries.shape[1]
    cap = 2 * tokens * routes.shape[1] // nsp
    slots = nsp * cap
    longest = ntp // 2
    chunks = nsp // (2 * CORES)
    vmem = pl.BlockSpec(memory_space=pltpu.VMEM)
    smem = pl.BlockSpec(memory_space=pltpu.SMEM)
    anywhere = pl.BlockSpec(memory_space=pl.ANY)
    dma = pltpu.SemaphoreType.DMA
    return pl.pallas_call(
        functools.partial(layer, nsp, ntp, cap),
        out_shape=jax.ShapeDtypeStruct((tokens, cols), BF16),
        in_specs=[anywhere] + [vmem] * 6 + [smem, vmem, vmem] + [anywhere] * 6,
        out_specs=vmem,
        scratch_shapes=[
            pltpu.VMEM((keys.shape[1], WINDOW), BF16),
            pltpu.VMEM((values.shape[1], WINDOW), BF16),
            pltpu.VMEM((1, WINDOW), jnp.int32),
            pltpu.VMEM((ntp * heads_wide, cols), BF16),
            pltpu.VMEM((tokens, cols), BF16),
            pltpu.VMEM((ntp, tokens, heads_wide), BF16),
            pltpu.VMEM((ntp, tokens, cols), BF16),
            pltpu.VMEM((ntp, tokens, cols), BF16),
            pltpu.VMEM((slots, tokens), BF16),
            pltpu.VMEM((2, tokens, slots), BF16),
            pltpu.VMEM((slots, cols), BF16),
            pltpu.VMEM((ntp, (2 * CORES - 1) * cap, cols), BF16),
            pltpu.VMEM((ntp, 8, tokens), F32),
            pltpu.VMEM((ntp, slots, cols), BF16),
            pltpu.VMEM((ntp, slots + tokens, hidden), BF16),
            pltpu.VMEM((slots, cols), BF16),
            pltpu.VMEM((slots, cols), BF16),
            pltpu.VMEM((width, 2 * hidden), BF16),
            pltpu.VMEM((ntp * hidden, cols), BF16),
            pltpu.VMEM((width, 2 * hidden), BF16),
            pltpu.VMEM((ntp * hidden, cols), BF16),
            dma((3,)),
            dma((3,)),
            dma((ntp - 1,)),
            dma((ntp - 1,)),
            dma((ntp - 1,)),
            dma((ntp - 1,)),
            dma,
            dma((tokens // WINDOW, 2, longest)),
            dma,
            dma((tokens // WINDOW, 2, longest)),
            dma((ntp - 1,)),
            dma((ntp - 1,)),
            dma,
            dma,
            dma((nsp,)),
            dma,
            dma((chunks, 2, longest)),
            dma,
            dma((chunks + 1, 2, longest)),
            dma,
            dma((nsp,)),
            dma((7,)),
            pltpu.SemaphoreType.REGULAR,
            pltpu.SemaphoreType.REGULAR,
        ],
        compiler_params=pltpu.CompilerParams(collective_id=0, has_side_effects=True),
        name="layer",
    )(
        residual,
        queries,
        keys.T,
        values.T,
        segments.reshape(1, tokens),
        routes.T,
        route_weight.T,
        sinks,
        out_weight,
        norm_gain.reshape(1, width),
        expert_gate,
        expert_up,
        expert_down,
        shared_gate,
        shared_up,
        shared_down,
    )


def solution(mesh):
    in_specs = (
        P(GRP_SP, None),
        P(GRP_SP, "tp"),
        P(GRP_SP, "tp"),
        P(GRP_SP, "tp"),
        P(GRP_SP),
        P(GRP_SP, None),
        P(GRP_SP, None),
        P("tp"),
        P("tp", None),
        P(),
        P("sp", None, "tp"),
        P("sp", None, "tp"),
        P("sp", None, "tp"),
        P(None, "tp"),
        P(None, "tp"),
        P(None, "tp"),
    )
    return jax.shard_map(
        functools.partial(shards, mesh.shape["sp"], mesh.shape["tp"]),
        mesh=mesh,
        in_specs=in_specs,
        out_specs=P(GRP_SP, "tp"),
        check_vma=False,
    )
```
